128 devices in a mesh: rep: 2 (over z_hi), fs: 32 (over z_lo, y, x), tp: 2 (over core).
Axes of the slice: x: 4, y: 4, z: 4 (z_hi: 2, z_lo: 2; z = z_hi * 2 + z_lo), core: 2. Of those that a mesh axis runs over, the one named last changes fastest.
Arguments:
- tokens: bfloat16 [65536, 2048], P(('rep', 'fs'), 'tp'), may hold values from -13 to 13
- norm_gains: float32 [4, 2048], replicated, may hold values from 0.1 to 1.9
- mix_weight: float32 [2048, 2048], P('fs', 'tp'), may hold values from -0.125 to 0.125
- mix_scale: float32 [32, 64], P('tp', 'fs'), may hold values from 0.5 to 2
- group_weight: float32 [4, 512, 512], P('tp', 'fs'), may hold values from -0.25 to 0.25
- group_scale: float32 [32, 64], P('tp', 'fs'), may hold values from 0.35 to 2.9
- up_weight: float32 [2048, 4096], P('fs', 'tp'), may hold values from -0.125 to 0.125
- up_scale: float32 [64, 64], P('tp', 'fs'), may hold values from 0.5 to 2
- down_weight: float32 [4096, 2048], P('tp', 'fs'), may hold values from -0.09375 to 0.09375
- down_scale: float32 [32, 64], P('tp', 'fs'), may hold values from 0.35 to 2.9
Outputs:
- layer_out: bfloat16 [65536, 2048], P(('rep', 'fs'), 'tp')
The draws below stay inside these ranges and needn't reach their ends.
All inputs are finite; a program needn't handle non-finite values.
Results may differ from the reference program's by a relative error of at most 0.0083.
Values may be sent and summed in bfloat16 or wider, within the bound.
A program may use at most 128 MiB of HBM per device.

```python
import math
import jax
import jax.numpy as jnp
from jax import lax

D = 2048
GROUPS = 4
GW = 512
FF = 4096
LENGTH = 1024
TOKENS = 65536
N_TP = 2


def draw_tokens(key, part):
    noise_key, column_key = jax.random.split(jax.random.fold_in(key, 11))
    base = jnp.clip(jax.random.normal(noise_key, (TOKENS, D), jnp.float32), -4.0, 4.0)
    column = 10.0 ** jax.random.uniform(column_key, (1, D), jnp.float32, -0.5, 0.5)
    return (base * column).astype(jnp.bfloat16)


def ramp_scale(key, height):
    spread = 10.0 ** jax.random.uniform(key, (height, 64), jnp.float32, -0.15, 0.15)
    rising = 4.0 ** (jnp.arange(height, dtype=jnp.float32)[:, None] / (height - 1) - 0.5)
    return spread * rising


def draw_group_scale(key, part):
    return ramp_scale(jax.random.fold_in(key, 21), D // 64)


def draw_down_scale(key, part):
    return ramp_scale(jax.random.fold_in(key, 31), D // 64)


def level_of(stream_key, dims, shards, low, high):
    gain, own = 1.0, jax.random.fold_in(stream_key, 6)
    for dim, parts in shards:
        steps = jnp.exp(jax.random.uniform(jax.random.fold_in(own, dim), (parts,), jnp.float32, low / len(shards), high / len(shards)))
        gain = gain * jnp.repeat(steps, dims[dim] // parts).reshape([-1 if axis == dim else 1 for axis in range(len(dims))])
    return gain


def bell_draw(rng, dims, width, limit, shards=(), kind=jnp.bfloat16):
    values = jax.random.normal(rng, dims, jnp.float32) * width
    if len(shards) > 0:
        values = level_of(rng, dims, shards, -0.22, 0.18) * values
    return jnp.clip(values, min=-limit, max=limit).astype(kind)


def setup_inputs(seed: int = 0) -> dict:
    key_of = jax.random.split(jax.random.key(seed), 11)
    return {
        "tokens": draw_tokens(jax.random.fold_in(key_of[10], 71), 0),
        "norm_gains": jnp.clip(1.0 + 0.18 * jax.random.normal(key_of[1], (4, D), jnp.float32), 0.1, 1.9),
        "mix_weight": bell_draw(key_of[2], (D, D), D ** -0.5, 0.125, ((0, 32), (1, 2)), jnp.float32),
        "mix_scale": jnp.clip(jnp.exp(math.log(2.0) - 1.3862944 * jax.random.uniform(key_of[3], (D // 64, 64), jnp.float32) ** level_of(key_of[3], (D // 64, 64), ((0, 2), (1, 32)), -0.2, 0.2)), 0.5, 2.0),
        "group_weight": bell_draw(key_of[4], (GROUPS, GW, GW), GW ** -0.5, 0.25, ((0, 2), (1, 32)), jnp.float32),
        "group_scale": draw_group_scale(jax.random.fold_in(key_of[10], 71), 0),
        "up_weight": bell_draw(key_of[6], (D, FF), D ** -0.5, 0.125, ((0, 32), (1, 2)), jnp.float32),
        "up_scale": jnp.clip(jnp.exp(math.log(2.0) - 1.3862944 * jax.random.uniform(key_of[7], (FF // 64, 64), jnp.float32) ** level_of(key_of[7], (FF // 64, 64), ((0, 2), (1, 32)), -0.2, 0.2)), 0.5, 2.0),
        "down_weight": bell_draw(key_of[8], (FF, D), FF ** -0.5, 0.09375, ((0, 2), (1, 32)), jnp.float32),
        "down_scale": draw_down_scale(jax.random.fold_in(key_of[10], 71), 0),
    }


epsilon = 1e-06

def rounded(values):
    return lax.optimization_barrier(values.astype(jnp.bfloat16)).astype(jnp.float32)

def inverse_rms(values):
    return lax.rsqrt(lax.optimization_barrier(jnp.mean(values * values, axis=1, keepdims=True)) + epsilon)

def pool_groups(mixed):
    length = mixed.shape[0]
    upward = mixed.astype(jnp.float32).reshape(length, GROUPS, GW)
    sums = jnp.concatenate([jnp.zeros((17, GROUPS, GW), jnp.float32), jnp.cumsum(upward, axis=0)], axis=0)
    position = jnp.arange(length, dtype=jnp.int32)
    pieces = []
    for group in range(GROUPS):
        window = 2 ** (group + 1)
        upper = sums[17:, group]
        lower = sums[17 - window:17 - window + length, group]
        count = jnp.minimum(position + 1, window).astype(jnp.float32)[:, None]
        pieces.append((upper - lower) / count - upward[:, group])
    return jnp.stack(pieces, axis=1).astype(jnp.bfloat16)

def reference(tokens, norm_gains, mix_weight, mix_scale, group_weight, group_scale, up_weight, up_scale, down_weight, down_scale):
    mix_matrix = mix_weight.astype(jnp.bfloat16)
    group_matrix = group_weight.astype(jnp.bfloat16).astype(jnp.float32)
    up_matrix = up_weight.astype(jnp.bfloat16)
    down_matrix = down_weight.astype(jnp.bfloat16)
    mix_cols = mix_scale.reshape(-1)
    group_cols = group_scale.reshape(-1)
    up_cols = up_scale.reshape(-1)
    down_cols = down_scale.reshape(-1)
    block = FF // N_TP

    def one_sequence(sequence):
        seq_float = sequence.astype(jnp.float32)
        normed = (seq_float * inverse_rms(seq_float) * norm_gains[0]).astype(jnp.bfloat16)
        mixed = (jnp.dot(normed, mix_matrix, preferred_element_type=jnp.float32) * mix_cols).astype(jnp.bfloat16)
        pooled = pool_groups(mixed)
        grouped = jnp.einsum('sgc,gcd->sgd', pooled.astype(jnp.float32), group_matrix).reshape(LENGTH, D)
        branch = rounded(grouped * group_cols)
        middle = (seq_float + rounded(branch * inverse_rms(branch) * norm_gains[1])).astype(jnp.bfloat16)
        mid_float = middle.astype(jnp.float32)
        normed_mid = (mid_float * inverse_rms(mid_float) * norm_gains[2]).astype(jnp.bfloat16)
        upward = jnp.dot(normed_mid, up_matrix, preferred_element_type=jnp.float32) * up_cols
        active = jnp.maximum(upward, 0.0)
        hidden = (active * active).astype(jnp.bfloat16)
        total = jnp.zeros((LENGTH, D), jnp.float32)
        for shard in range(N_TP):
            partial_term = jnp.dot(hidden[:, shard * block:(shard + 1) * block], down_matrix[shard * block:(shard + 1) * block], preferred_element_type=jnp.float32)
            total = total + rounded(partial_term)
        down = rounded(total * down_cols)
        return (mid_float + rounded(down * inverse_rms(down) * norm_gains[3])).astype(jnp.bfloat16)
    result = lax.map(one_sequence, tokens.reshape(-1, LENGTH, D))
    return result.reshape(-1, D)
```

```python
import functools

import jax
import jax.numpy as jnp
from jax import lax
from jax.experimental import pallas as pl
from jax.experimental.pallas import tpu as pltpu
from jax.sharding import Mesh
from jax.sharding import PartitionSpec as P

FS = ("fs_0", "fs_1", "fs_2")
REP_FS = ("rep", "fs_0", "fs_1", "fs_2")
MESH = pl.DeviceIdType.MESH
ORDERS = ("xyz", "yxz", "xzy", "yzx")
ALL = slice(None)
EPS = 1e-06

LENGTH = 1024
HALF = 1024
GW = 512
NB = 5
ROWS = (80, 64, 64, 64, 64)
BLOCK = 256
NR = LENGTH // BLOCK
F32, BF16 = jnp.float32, jnp.bfloat16


def dot(a, b):
    return jnp.dot(a, b, preferred_element_type=F32)


def dot_t(a, b):
    return lax.dot_general(a, b, (((1,), (1,)), ((), ())), preferred_element_type=F32)


def spot():
    return dict(
        z=lax.axis_index("rep") * 2 + lax.axis_index("fs_0"),
        y=lax.axis_index("fs_1"),
        x=lax.axis_index("fs_2"),
        t=lax.axis_index("tp"),
    )


def to(axis, at):
    if axis == "x":
        return {"fs_2": at}
    if axis == "y":
        return {"fs_1": at}
    if axis == "z":
        return {"rep": at // 2, "fs_0": at % 2}
    return {"tp": at}


def send(src, dst, send_sem, recv_sem, axis, at):
    return pltpu.make_async_remote_copy(
        src_ref=src,
        dst_ref=dst,
        send_sem=send_sem,
        recv_sem=recv_sem,
        device_id=to(axis, at),
        device_id_type=MESH,
    )


class Gather:
    def __init__(self, bufs, send_sem, recv_sem, me):
        self.bufs, self.send_sem, self.recv_sem, self.me = bufs, send_sem, recv_sem, me
        self.sent = []
        self.steps = {
            (b, c): self.plan(b, c, order)
            for b in range(len(bufs))
            for c, order in enumerate(ORDERS)
        }

    def region(self, b, c, at, half):
        lane = 256 * c + (128 * half if half is not None else 0)
        width = 256 if half is None else 128
        return self.bufs[b].at[at["z"], at["y"], at["x"], :, pl.ds(lane, width)]

    def copy(self, b, c, slot, ref, axis, at):
        return send(
            ref, ref, self.send_sem.at[b, c, slot], self.recv_sem.at[b, c, slot], axis, at
        )

    def plan(self, b, c, order):
        me = self.me
        own = dict(z=me["z"] % 2, y=me["y"], x=me["x"])
        steps, slot = [], 0
        for axis in order:
            up, down, far = (lax.rem(me[axis] + d, 4) for d in (1, 3, 2))

            def part(i, half=None, own=own, axis=axis):
                return self.region(b, c, {**own, axis: i}, half)

            if axis == "z":
                here, other = own["z"], 1 - own["z"]
                steps.append(
                    (
                        [(slot, part(here, 0), axis, up), (slot + 1, part(here, 1), axis, down)],
                        [(slot, part(other, 0)), (slot + 1, part(other, 1))],
                    )
                )
                slot += 2
            else:
                here = me[axis]
                steps.append(
                    (
                        [(slot, part(here), axis, up), (slot + 1, part(here), axis, down)],
                        [(slot, part(down)), (slot + 1, part(up))],
                    )
                )
                steps.append(
                    (
                        [
                            (slot + 2, part(down, 0), axis, up),
                            (slot + 3, part(up, 1), axis, down),
                        ],
                        [(slot + 2, part(far, 0)), (slot + 3, part(far, 1))],
                    )
                )
                slot += 4
            own = {**own, axis: ALL}
        return steps

    def tick(self, b, s, colours=range(4)):
        for c in colours:
            if s > 0:
                for slot, ref in self.steps[b, c][s - 1][1]:
                    self.copy(b, c, slot, ref, "x", self.me["x"]).wait_recv()
            if s < 5:
                for slot, ref, axis, at in self.steps[b, c][s][0]:
                    copy = self.copy(b, c, slot, ref, axis, at)
                    copy.start()
                    self.sent.append(copy)

    def finish(self):
        for copy in self.sent:
            copy.wait_send()


def greet(me):
    barrier = pltpu.get_barrier_semaphore()
    peers = [("x", 1), ("x", 2), ("x", 3), ("y", 1), ("y", 2), ("y", 3), ("z", 1), ("z", 3)]
    for axis, d in peers:
        pl.semaphore_signal(
            barrier, inc=1, device_id=to(axis, lax.rem(me[axis] + d, 4)), device_id_type=MESH
        )
    pl.semaphore_signal(barrier, inc=1, device_id=to("t", 1 - me["t"]), device_id_type=MESH)
    pl.semaphore_wait(barrier, len(peers) + 1)


def kernel(
    tokens,
    gains,
    mix_w,
    group_w,
    up_w,
    down_w,
    tile,
    out,
    w0,
    w1,
    w2,
    w3,
    w4,
    x_buf,
    normed,
    mixed,
    branch,
    hidden,
    acc,
    part_out,
    part_in,
    squares,
    band,
    sc_in,
    sc_sum,
    scale,
    g_send,
    g_recv,
    load_sem,
    p_send,
    p_recv,
    s_send,
    s_recv,
):
    me = spot()
    t, other = me["t"], 1 - me["t"]
    here = (me["z"] % 2, me["y"], me["x"])
    bufs = (w0, w1, w2, w3, w4)
    gather = Gather(bufs, g_send, g_recv, me)
    sent = []

    def rows_of(i, size=BLOCK):
        return pl.ds(i * size, size)

    loads = []
    for i in range(NR):
        load = pltpu.make_async_copy(
            tokens.at[rows_of(i)], x_buf.at[t, rows_of(i)], load_sem.at[i]
        )
        load.start()
        loads.append(load)
    w0[here[0], here[1], here[2], 0:64] = mix_w[...].astype(BF16)
    w0[here[0], here[1], here[2], 64:80, 0:GW] = group_w[0].astype(BF16)
    w0[here[0], here[1], here[2], 64:80, GW:] = group_w[1].astype(BF16)
    greet(me)

    def share(kind, i, src, dst):
        copy = send(src, dst, p_send.at[kind, i], p_recv.at[kind, i], "t", other)
        copy.start()
        sent.append(copy)

    def arrived(kind, i, ref):
        send(ref, ref, p_send.at[kind, i], p_recv.at[kind, i], "t", other).wait_recv()

    gather.tick(0, 0)
    for i in range(NR):
        share(0, i, tokens.at[rows_of(i)], x_buf.at[t, rows_of(i)])

    def scale_send(slot, src, axis, at):
        copy = send(src, sc_in.at[slot], s_send.at[slot], s_recv.at[slot], axis, at)
        copy.start()
        sent.append(copy)

    def scale_wait(slot):
        send(sc_in.at[slot], sc_in.at[slot], s_send.at[slot], s_recv.at[slot], "t", other).wait_recv()

    def scales(step):
        if step == 0:
            for d in (1, 2, 3):
                scale_send(d - 1, tile, "x", lax.rem(me["x"] + d, 4))
        if step == 1:
            for d in (1, 2, 3):
                scale_wait(d - 1)
            sc_sum[0] = tile[...] + sc_in[0] + sc_in[1] + sc_in[2]
        if step == 2:
            for d in (1, 2, 3):
                scale_send(d + 2, sc_sum.at[0], "y", lax.rem(me["y"] + d, 4))
        if step == 3:
            for d in (1, 2, 3):
                scale_wait(d + 2)
            sc_sum[1] = sc_sum[0] + sc_in[3] + sc_in[4] + sc_in[5]
        if step == 4:
            scale_send(6, sc_sum.at[1], "z", me["z"] + 1 - 2 * (me["z"] % 2))
        if step == 5:
            scale_wait(6)
            whole = sc_sum[1] + sc_in[6]
            for q in range(40):
                scale[q // 8 : q // 8 + 1, 128 * (q % 8) : 128 * (q % 8) + 128] = whole[q : q + 1]

    def fill():
        up = up_w[...].astype(BF16)
        w1[here[0], here[1], here[2]] = up[:, 0:1024]
        w2[here[0], here[1], here[2]] = up[:, 1024:]
        eye = (
            lax.broadcasted_iota(jnp.int32, (64, 64), 0)
            == lax.broadcasted_iota(jnp.int32, (64, 64), 1)
        ).astype(BF16)
        turned = dot_t(eye, down_w[...].astype(BF16)).astype(BF16)
        w3[here[0], here[1], here[2]] = turned[:, 0:1024]
        w4[here[0], here[1], here[2]] = turned[:, 1024:]

    def bands():
        i = lax.broadcasted_iota(jnp.int32, (BLOCK, 2 * BLOCK), 0)
        j = lax.broadcasted_iota(jnp.int32, (BLOCK, 2 * BLOCK), 1) - BLOCK
        for g, window in enumerate((2 + 6 * t, 4 + 12 * t)):
            band[g] = jnp.where((j <= i) & (j > i - window), 1.0, 0.0).astype(BF16)

    def mean_inverse(total):
        return lax.rsqrt(total * (1.0 / (2 * HALF)) + EPS)

    def row_sum(v):
        return jnp.sum(v, axis=1, keepdims=True)

    SUB = 16

    def first_norm(i):
        loads[i].wait()
        arrived(0, i, x_buf.at[other, rows_of(i)])
        g0, g1 = gains[0:1, 0:HALF], gains[0:1, HALF:]

        def body(k, _):
            rows = pl.ds(pl.multiple_of(i * BLOCK + k * SUB, SUB), SUB)
            a, b = x_buf[0, rows].astype(F32), x_buf[1, rows].astype(F32)
            inverse = mean_inverse(row_sum(a * a + b * b))
            normed[rows, 0:HALF] = (a * inverse * g0).astype(BF16)
            normed[rows, HALF:] = (b * inverse * g1).astype(BF16)
            return 0

        lax.fori_loop(0, BLOCK // SUB, body, 0, unroll=2)

    def mix(c):
        cols = slice(256 * c, 256 * c + 256)
        weight = w0[:, :, :, 0:64, cols].reshape(2 * HALF, 256)

        def body(i, _):
            rows = pl.ds(pl.multiple_of(i * 512, 512), 512)
            mixed[rows, cols] = (dot(normed[rows], weight) * scale[0:1, cols]).astype(BF16)
            return 0

        lax.fori_loop(0, 2, body, 0)

    def pool(i):
        rows = slice(i * BLOCK, i * BLOCK + BLOCK)
        for g in range(2):
            cols = slice(GW * g, GW * g + GW)
            window = (2 + 6 * t, 4 + 12 * t)[g]
            own = mixed[rows, cols]
            if i == 0:
                sums = dot(band[g, :, BLOCK:], own)
                position = lax.broadcasted_iota(jnp.int32, (BLOCK, 1), 0)
                sums = sums / jnp.minimum(position + 1, window).astype(F32)
            else:
                sums = dot(band[g], mixed[rows.start - BLOCK : rows.stop, cols])
                sums = sums * (1.0 / jnp.full((BLOCK, 1), window, jnp.int32).astype(F32))
            pooled = (sums - own.astype(F32)).astype(BF16)
            weight = w0[:, :, :, 64:80, cols].reshape(GW, GW)
            branch[t, rows, cols] = (dot(pooled, weight) * scale[1:2, cols]).astype(BF16)

    def branch_share(i):
        share(1, i, branch.at[t, rows_of(i)], branch.at[t, rows_of(i)])

    def middle(i):
        arrived(1, i, branch.at[other, rows_of(i)])
        post = [gains[1:2, 0:HALF], gains[1:2, HALF:]]
        pre = [gains[2:3, 0:HALF], gains[2:3, HALF:]]

        def body(k, _):
            rows = pl.ds(pl.multiple_of(i * BLOCK + k * SUB, SUB), SUB)
            parts = [branch[h, rows].astype(F32) for h in range(2)]
            inverse = mean_inverse(row_sum(parts[0] * parts[0] + parts[1] * parts[1]))
            mids = []
            for h in range(2):
                add = (parts[h] * inverse * post[h]).astype(BF16).astype(F32)
                mid = (x_buf[h, rows].astype(F32) + add).astype(BF16)
                x_buf[h, rows] = mid
                mids.append(mid.astype(F32))
            inverse = mean_inverse(row_sum(mids[0] * mids[0] + mids[1] * mids[1]))
            for h in range(2):
                normed[rows, h * HALF : h * HALF + HALF] = (mids[h] * inverse * pre[h]).astype(BF16)
            return 0

        lax.fori_loop(0, BLOCK // SUB, body, 0, unroll=2)

    def up(b, c):
        cols = slice(256 * c, 256 * c + 256)
        place = slice((b - 1) * 1024 + 256 * c, (b - 1) * 1024 + 256 * c + 256)
        weight = bufs[b][:, :, :, :, cols].reshape(2 * HALF, 256)

        def body(i, _):
            rows = pl.ds(pl.multiple_of(i * 512, 512), 512)
            act = jnp.maximum(dot(normed[rows], weight) * scale[b + 1 : b + 2, cols], 0.0)
            hidden[rows, place] = (act * act).astype(BF16)
            return 0

        lax.fori_loop(0, 2, body, 0)

    def down_first(i):
        rows = pl.ds(i * 512, 512)
        left = hidden[rows, 0:1024]

        def body(k, _):
            weight = w3[k // 4, k % 4].reshape(256, 1024)
            acc[k // 4, rows, pl.ds(pl.multiple_of(k % 4 * 256, 256), 256)] = dot_t(left, weight)
            return 0

        lax.fori_loop(0, 8, body, 0)

    def down_second(i, half, target):
        rows = pl.ds(i * BLOCK, BLOCK)
        left = hidden[rows, 1024:]

        def body(k, _):
            weight = w4[half, k].reshape(256, 1024)
            cols = pl.ds(pl.multiple_of(k * 256, 256), 256)
            target[rows, cols] = (acc[half, rows, cols] + dot_t(left, weight)).astype(BF16)
            return 0

        lax.fori_loop(0, 4, body, 0)

    def part_share(i):
        share(2, i, part_out.at[rows_of(i)], part_in.at[rows_of(i)])

    def total(i):
        arrived(2, i, part_in.at[rows_of(i)])

        def body(k, _):
            rows = pl.ds(pl.multiple_of(i * BLOCK + k * SUB, SUB), SUB)
            both = mixed[rows].astype(F32) + part_in[rows].astype(F32)
            down = (both * scale[4:5]).astype(BF16)
            mixed[rows] = down
            down = down.astype(F32)
            square = down * down
            lanes = square[:, 0:128]
            for q in range(1, 8):
                lanes = lanes + square[:, 128 * q : 128 * q + 128]
            squares[t, rows] = lanes
            return 0

        lax.fori_loop(0, BLOCK // SUB, body, 0, unroll=2)
        share(3, i, squares.at[t, rows_of(i)], squares.at[t, rows_of(i)])

    def final(i):
        arrived(3, i, squares.at[other, rows_of(i)])
        gain = gains[3:4, pl.ds(pl.multiple_of(t * HALF, HALF), HALF)]

        def body(k, _):
            rows = pl.ds(pl.multiple_of(i * BLOCK + k * SUB, SUB), SUB)
            inverse = mean_inverse(row_sum(squares[0, rows] + squares[1, rows]))
            add = (mixed[rows].astype(F32) * inverse * gain).astype(BF16).astype(F32)
            out[rows] = (x_buf[t, rows].astype(F32) + add).astype(BF16)
            return 0

        lax.fori_loop(0, BLOCK // SUB, body, 0, unroll=2)

    def round_(k):
        for b in range(NB):
            if 0 <= k - b <= 5:
                gather.tick(b, k - b)

    scales(0)
    fill()
    round_(1)
    scales(1)
    bands()
    scales(2)
    round_(2)
    for i in range(NR):
        first_norm(i)
    round_(3)
    scales(3)
    round_(4)
    scales(4)
    round_(5)
    scales(5)
    for c in range(4):
        mix(c)
    round_(6)
    for i in range(NR):
        pool(i)
        branch_share(i)
    for i in range(NR):
        middle(i)
    round_(7)
    for c in range(4):
        up(1, c)
    for c in range(4):
        up(2, c)
    round_(8)
    for i in range(2):
        down_first(i)
    round_(9)
    for i in range(NR):
        down_second(i, other, part_out)
        part_share(i)
    for i in range(NR):
        down_second(i, t, mixed)
    for i in range(NR):
        total(i)
    for i in range(NR):
        final(i)
    gather.finish()
    for copy in sent:
        copy.wait_send()


def on_device(
    tokens,
    norm_gains,
    mix_weight,
    mix_scale,
    group_weight,
    group_scale,
    up_weight,
    up_scale,
    down_weight,
    down_scale,
):
    place = lax.axis_index(FS)
    scales = jnp.concatenate([mix_scale, group_scale, up_scale, down_scale], axis=0)
    own = (jnp.arange(32, dtype=jnp.int32) == place)[None, None, :, None]
    tile = jnp.where(own, scales.reshape(40, 2, 1, 2), 0.0).reshape(40, 128)
    vmem = pl.BlockSpec(memory_space=pltpu.VMEM)
    dma = pltpu.SemaphoreType.DMA
    return pl.pallas_call(
        kernel,
        out_shape=jax.ShapeDtypeStruct((LENGTH, HALF), BF16),
        in_specs=[pl.BlockSpec(memory_space=pl.ANY)] + [vmem] * 6,
        out_specs=vmem,
        scratch_shapes=[pltpu.VMEM((2, 4, 4, r, 1024), BF16) for r in ROWS]
        + [
            pltpu.VMEM((2, LENGTH, HALF), BF16),
            pltpu.VMEM((LENGTH, 2 * HALF), BF16),
            pltpu.VMEM((LENGTH, HALF), BF16),
            pltpu.VMEM((2, LENGTH, HALF), BF16),
            pltpu.VMEM((LENGTH, 2048), BF16),
            pltpu.VMEM((2, LENGTH, HALF), F32),
            pltpu.VMEM((LENGTH, HALF), BF16),
            pltpu.VMEM((LENGTH, HALF), BF16),
            pltpu.VMEM((2, LENGTH, 128), F32),
            pltpu.VMEM((2, BLOCK, 2 * BLOCK), BF16),
            pltpu.VMEM((7, 40, 128), F32),
            pltpu.VMEM((2, 40, 128), F32),
            pltpu.VMEM((5, 1024), F32),
            dma((NB, 4, 10)),
            dma((NB, 4, 10)),
            dma((NR,)),
            dma((4, NR)),
            dma((4, NR)),
            dma((7,)),
            dma((7,)),
        ],
        compiler_params=pltpu.CompilerParams(
            collective_id=0, has_side_effects=True, vmem_limit_bytes=67_000_000
        ),
    )(tokens, norm_gains, mix_weight, group_weight, up_weight, down_weight, tile)


def solution(mesh):
    finer = Mesh(
        mesh.devices.reshape(mesh.shape["rep"], 2, 4, 4, mesh.shape["tp"]),
        ("rep", "fs_0", "fs_1", "fs_2", "tp"),
    )
    in_specs = (
        P(REP_FS, "tp"),
        P(),
        P(FS, "tp"),
        P("tp", FS),
        P("tp", FS, None),
        P("tp", FS),
        P(FS, "tp"),
        P("tp", FS),
        P("tp", FS),
        P("tp", FS),
    )
    out_specs = P(REP_FS, "tp")
    return jax.shard_map(
        on_device, mesh=finer, in_specs=in_specs, out_specs=out_specs, check_vma=False
    )
```

```python
import functools

import jax
import jax.numpy as jnp
from jax import lax
from jax.experimental import pallas as pl
from jax.experimental.pallas import tpu as pltpu
from jax.sharding import Mesh
from jax.sharding import PartitionSpec as P

FS = ("fs_0", "fs_1", "fs_2")
REP_FS = ("rep", "fs_0", "fs_1", "fs_2")
MESH = pl.DeviceIdType.MESH
ALL = slice(None)
EPS = 1e-06

LENGTH = 1024
HALF = 1024
GW = 512
ROWS = (80, 64, 64, 64, 64)
BATCHES = ((0, 0, 256), (1, 0, 256), (2, 0, 256), (3, 0, 256), (4, 0, 128), (4, 512, 128))
NB = len(BATCHES)
POOL = 56
LAG = 20
MROWS = 512
BLOCK = 256
NR = LENGTH // BLOCK
F32, BF16 = jnp.float32, jnp.bfloat16


PLAN = (
    ("T", 1, 1, 0), ("T", 1, 0, 0), ("T", 1, 2, 0), ("T", 1, 3, 0), ("bands",), ("T", 3, 1, 0),
    ("T", 3, 0, 0), ("T", 3, 3, 0), ("T", 3, 2, 0), ("T", 4, 1, 0), ("T", 4, 0, 0), ("T", 5, 1, 0),
    ("T", 4, 2, 0), ("T", 4, 3, 0), ("T", 5, 0, 0), ("T", 5, 3, 0), ("T", 5, 2, 0), ("T", 2, 1, 0),
    ("T", 2, 0, 0), ("T", 0, 1, 1), ("T", 0, 0, 1), ("sc", 1), ("sc", 2), ("norm", 0), ("T", 0, 2, 1),
    ("T", 1, 1, 1), ("T", 0, 3, 1), ("T", 1, 0, 1), ("T", 2, 2, 0), ("T", 2, 3, 0), ("norm", 1),
    ("T", 1, 2, 1), ("T", 1, 3, 1), ("norm", 2), ("T", 3, 1, 1), ("T", 3, 0, 1), ("T", 3, 2, 1),
    ("T", 3, 3, 1), ("norm", 3), ("T", 4, 1, 1), ("T", 4, 0, 1), ("T", 4, 2, 1), ("T", 5, 1, 1),
    ("T", 4, 3, 1), ("T", 5, 0, 1), ("sc", 3), ("T", 5, 2, 1), ("T", 5, 3, 1), ("sc", 4), ("T", 2, 1, 1),
    ("T", 2, 0, 1), ("T", 0, 1, 2), ("T", 0, 0, 2), ("T", 1, 1, 2), ("T", 0, 2, 2), ("T", 0, 3, 2),
    ("T", 1, 0, 2), ("T", 1, 3, 2), ("T", 1, 2, 2), ("sc", 5), ("T", 3, 0, 2), ("T", 3, 1, 2),
    ("T", 3, 2, 2), ("T", 0, 2, 3), ("T", 3, 3, 2), ("T", 0, 0, 3), ("T", 0, 1, 3), ("T", 0, 3, 3),
    ("T", 4, 1, 2), ("T", 4, 0, 2), ("T", 4, 2, 2), ("T", 4, 3, 2), ("T", 5, 2, 2), ("T", 5, 3, 2),
    ("T", 1, 0, 3), ("T", 1, 1, 3), ("T", 1, 2, 3), ("T", 1, 3, 3), ("T", 0, 1, 4), ("T", 0, 2, 4),
    ("T", 0, 0, 4), ("T", 0, 3, 4), ("T", 2, 3, 1), ("T", 2, 2, 1), ("T", 1, 0, 4), ("T", 1, 1, 4),
    ("T", 2, 0, 2), ("T", 2, 1, 2), ("T", 0, 1, 5), ("mix", 1), ("T", 1, 2, 4), ("T", 1, 3, 4),
    ("T", 3, 0, 3), ("T", 3, 1, 3), ("T", 3, 2, 3), ("T", 3, 3, 3), ("T", 0, 0, 5), ("mix", 0),
    ("T", 2, 2, 2), ("T", 2, 3, 2), ("T", 0, 2, 5), ("mix", 2), ("T", 0, 3, 5), ("mix", 3), ("T", 2, 1, 3),
    ("T", 2, 0, 3), ("pool", 0), ("share", 0), ("pool", 1), ("share", 1), ("pool", 2), ("share", 2),
    ("pool", 3), ("T", 3, 1, 4), ("share", 3), ("mid", 0), ("T", 5, 1, 2), ("T", 5, 0, 2), ("T", 3, 0, 4),
    ("T", 5, 2, 3), ("T", 5, 3, 3), ("mid", 1), ("mid", 2), ("T", 2, 2, 3), ("T", 2, 3, 3), ("T", 2, 1, 4),
    ("mid", 3), ("T", 2, 0, 4), ("T", 3, 2, 4), ("T", 3, 3, 4), ("T", 1, 0, 5), ("up", 1, 0),
    ("T", 1, 1, 5), ("up", 1, 1), ("T", 1, 2, 5), ("up", 1, 2), ("T", 1, 3, 5), ("up", 1, 3),
    ("T", 4, 1, 3), ("T", 4, 0, 3), ("T", 2, 2, 4), ("T", 2, 3, 4), ("T", 4, 2, 3), ("T", 5, 1, 3),
    ("T", 4, 3, 3), ("T", 5, 0, 3), ("T", 5, 2, 4), ("T", 5, 3, 4), ("T", 3, 0, 5), ("T", 3, 1, 5),
    ("T", 3, 2, 5), ("T", 3, 3, 5), ("dn", 3, 0), ("dn", 3, 1), ("T", 4, 1, 4), ("T", 4, 0, 4),
    ("dn", 3, 2), ("T", 2, 1, 5), ("up", 2, 1), ("T", 2, 2, 5), ("up", 2, 2), ("T", 5, 1, 4),
    ("T", 2, 3, 5), ("up", 2, 3), ("T", 4, 2, 4), ("T", 4, 3, 4), ("T", 5, 0, 4), ("dn", 3, 3),
    ("T", 2, 0, 5), ("up", 2, 0), ("T", 4, 0, 5), ("T", 4, 1, 5), ("T", 4, 2, 5), ("T", 4, 3, 5),
    ("dn", 4, 0), ("dn", 4, 1), ("dn", 4, 2), ("dn", 4, 3), ("T", 5, 0, 5), ("T", 5, 1, 5), ("T", 5, 2, 5),
    ("T", 5, 3, 5), ("last", 0), ("last", 1), ("own", 0), ("total", 0), ("total", 1), ("own", 1),
    ("total", 2), ("total", 3), ("final", 0), ("final", 1), ("final", 2), ("final", 3),
)
ORDERS = (
    ("xyz", "yxz", "xzy", "yzx"),
    ("xyz", "yxz", "xzy", "yzx"),
    ("xyz", "yxz", "xzy", "yzx"),
    ("xyz", "yxz", "xzy", "yzx"),
    ("xzy", "yzx", "xzy", "yzx"),
    ("xyz", "yxz", "xzy", "yzx"),
)


def dot(a, b):
    return jnp.dot(a, b, preferred_element_type=F32)


def dot_t(a, b):
    return lax.dot_general(a, b, (((1,), (1,)), ((), ())), preferred_element_type=F32)


def spot():
    return dict(
        z=lax.axis_index("rep") * 2 + lax.axis_index("fs_0"),
        y=lax.axis_index("fs_1"),
        x=lax.axis_index("fs_2"),
        t=lax.axis_index("tp"),
    )


def to(axis, at):
    if axis == "x":
        return {"fs_2": at}
    if axis == "y":
        return {"fs_1": at}
    if axis == "z":
        return {"rep": at // 2, "fs_0": at % 2}
    return {"tp": at}


def send(src, dst, send_sem, recv_sem, axis, at):
    return pltpu.make_async_remote_copy(
        src_ref=src,
        dst_ref=dst,
        send_sem=send_sem,
        recv_sem=recv_sem,
        device_id=to(axis, at),
        device_id_type=MESH,
    )


class Gather:
    def __init__(self, bufs, send_sem, recv_sem, me):
        self.bufs, self.send_sem, self.recv_sem, self.me = bufs, send_sem, recv_sem, me
        self.sent, self.ticks, self.free = [], 0, list(range(POOL))
        self.steps = {
            (b, c): self.plan(b, c, order)
            for b in range(NB)
            for c, order in enumerate(ORDERS[b])
        }

    def region(self, b, c, at, half):
        buf, lane, width = BATCHES[b]
        lane, rows = lane + width * c, ALL
        if half is not None and width == 256:
            lane, width = lane + 128 * half, 128
        elif half is not None:
            rows = pl.ds(32 * half, 32)
        return self.bufs[buf].at[at["z"], at["y"], at["x"], rows, pl.ds(lane, width)]

    def copy(self, b, c, k, pool, src, dst, axis, at):
        recv_sem = self.recv_sem.at[b, c, k]
        return send(src, dst, self.send_sem.at[pool], recv_sem, axis, at)

    def plan(self, b, c, order):
        me = self.me
        own = dict(z=me["z"] % 2, y=me["y"], x=me["x"])
        steps = []
        for axis in order:
            up, down, far = (lax.rem(me[axis] + d, 4) for d in (1, 3, 2))

            def part(i, half=None, own=own, axis=axis):
                return self.region(b, c, {**own, axis: i}, half)

            if axis == "z":
                here, other = own["z"], 1 - own["z"]
                steps.append(([(part(here, 0), axis, up), (part(here, 1), axis, down)], part(other)))
            else:
                here = me[axis]
                two = self.region(b, c, {**own, axis: pl.ds(0, 2)}, None)
                steps.append(([(part(here), axis, up), (part(here), axis, down)], two))
                steps.append(([(part(down, 0), axis, up), (part(up, 1), axis, down)], part(far)))
            own = {**own, axis: ALL}
        return steps

    def tick(self, b, c, s):
        self.ticks += 1
        while self.sent and self.sent[0][0] < self.ticks - LAG:
            self.release()
        if s > 0:
            ref = self.steps[b, c][s - 1][1]
            self.copy(b, c, s - 1, 0, ref, ref, "x", self.me["x"]).wait_recv()
        if s < 5:
            for ref, axis, at in self.steps[b, c][s][0]:
                if not self.free:
                    self.release()
                pool = self.free.pop(0)
                copy = self.copy(b, c, s, pool, ref, ref, axis, at)
                copy.start()
                self.sent.append((self.ticks, pool, copy))

    def release(self):
        _, pool, copy = self.sent.pop(0)
        copy.wait_send()
        self.free.append(pool)

    def finish(self):
        while self.sent:
            self.release()


def greet(me, wait):
    barrier = pltpu.get_barrier_semaphore()
    peers = [("x", 1), ("x", 2), ("x", 3), ("y", 1), ("y", 2), ("y", 3), ("z", 1), ("z", 3)]
    if wait:
        pl.semaphore_wait(barrier, len(peers) + 1)
        return
    for axis, d in peers:
        pl.semaphore_signal(
            barrier, inc=1, device_id=to(axis, lax.rem(me[axis] + d, 4)), device_id_type=MESH
        )
    pl.semaphore_signal(barrier, inc=1, device_id=to("t", 1 - me["t"]), device_id_type=MESH)


def kernel(
    tokens,
    gains_in,
    mix_in,
    group_in,
    up_in,
    down_in,
    mix_s_in,
    group_s_in,
    up_s_in,
    down_s_in,
    out,
    gains,
    mix_w,
    group_w,
    up_w,
    down_w,
    mix_s,
    group_s,
    up_s,
    down_s,
    w0,
    w1,
    w2,
    w3,
    w4,
    x_buf,
    normed,
    mixed,
    branch,
    hidden,
    acc,
    part_out,
    part_in,
    squares,
    band,
    tile,
    sc_in,
    sc_sum,
    scale,
    inverses,
    g_send,
    g_recv,
    load_sem,
    p_send,
    p_recv,
    s_send,
    s_recv,
    out_sem,
):
    me = spot()
    greet(me, False)
    t, other = me["t"], 1 - me["t"]
    here = (me["z"] % 2, me["y"], me["x"])
    bufs = (w0, w1, w2, w3, w4)
    gather = Gather(bufs, g_send, g_recv, me)
    sent, outs = [], []

    def rows_of(i, size=BLOCK):
        return pl.ds(i * size, size)

    def scale_tile():
        place = me["z"] % 2 * 16 + me["y"] * 4 + me["x"]
        lane = lax.broadcasted_iota(jnp.int32, (1, 128), 1)
        base = 0
        for ref in (mix_s, group_s, up_s, down_s):
            n = ref.shape[1] // 2
            q = lax.broadcasted_iota(jnp.int32, (n, 2 * n), 0)
            r = lax.broadcasted_iota(jnp.int32, (n, 2 * n), 1)
            value = jnp.zeros((n, 128), F32)
            for j in range(2):
                for h in range(2):
                    own = jnp.where(r == 2 * q + h, ref[j : j + 1], 0.0)
                    column = jnp.sum(own, axis=1, keepdims=True)
                    value = value + jnp.where(lane == h * 64 + 2 * place + j, column, 0.0)
            tile[base : base + n] = value
            base += n

    def load(k, src, dst):
        copy = pltpu.make_async_copy(src, dst, load_sem.at[k])
        copy.start()
        return copy

    pairs = (
        (mix_in, mix_w),
        (group_in, group_w),
        (mix_s_in, mix_s),
        (group_s_in, group_s),
        (up_s_in, up_s),
        (down_s_in, down_s),
        (up_in, up_w),
        (down_in, down_w),
        (gains_in, gains),
    )
    early = [load(k, src, dst) for k, (src, dst) in enumerate(pairs)]
    loads = [
        load(len(pairs) + i, tokens.at[rows_of(i)], x_buf.at[t, rows_of(i)]) for i in range(NR)
    ]
    for copy in early[:6]:
        copy.wait()
    w0[here[0], here[1], here[2], 0:64] = mix_w[...].astype(BF16)
    w0[here[0], here[1], here[2], 64:80, 0:GW] = group_w[0].astype(BF16)
    w0[here[0], here[1], here[2], 64:80, GW:] = group_w[1].astype(BF16)
    scale_tile()
    for copy in early[6:]:
        copy.wait()
    up_all, down_all = up_w[...].astype(BF16), down_w[...].astype(BF16)
    for ref, lane in ((w1, 0), (w2, 1024)):
        ref[here[0], here[1], here[2]] = up_all[:, lane : lane + 1024]
    for ref, lane in ((w3, 0), (w4, 1024)):
        ref[here[0], here[1], here[2]] = down_all[:, lane : lane + 1024]
    with jax.named_scope("greet"):
        greet(me, True)

    def share(kind, i, src, dst):
        copy = send(src, dst, p_send.at[kind, i], p_recv.at[kind, i], "t", other)
        copy.start()
        sent.append(copy)

    def arrived(kind, i, ref):
        send(ref, ref, p_send.at[kind, i], p_recv.at[kind, i], "t", other).wait_recv()

    for c in range(4):
        gather.tick(0, c, 0)
    for i in range(NR):
        share(0, i, tokens.at[rows_of(i)], x_buf.at[t, rows_of(i)])

    def scale_send(slot, src, axis, at):
        copy = send(src, sc_in.at[slot], s_send.at[slot], s_recv.at[slot], axis, at)
        copy.start()
        sent.append(copy)

    def scale_wait(slot):
        send(sc_in.at[slot], sc_in.at[slot], s_send.at[slot], s_recv.at[slot], "t", other).wait_recv()

    def scales(step):
        if step == 0:
            for d in (1, 2, 3):
                scale_send(d - 1, tile, "x", lax.rem(me["x"] + d, 4))
        if step == 1:
            for d in (1, 2, 3):
                scale_wait(d - 1)
            sc_sum[0] = tile[...] + sc_in[0] + sc_in[1] + sc_in[2]
        if step == 2:
            for d in (1, 2, 3):
                scale_send(d + 2, sc_sum.at[0], "y", lax.rem(me["y"] + d, 4))
        if step == 3:
            for d in (1, 2, 3):
                scale_wait(d + 2)
            sc_sum[1] = sc_sum[0] + sc_in[3] + sc_in[4] + sc_in[5]
        if step == 4:
            scale_send(6, sc_sum.at[1], "z", me["z"] + 1 - 2 * (me["z"] % 2))
        if step == 5:
            scale_wait(6)
            whole = sc_sum[1] + sc_in[6]
            for q in range(40):
                scale[q // 8 : q // 8 + 1, 128 * (q % 8) : 128 * (q % 8) + 128] = whole[q : q + 1]

    def bands():
        i = lax.broadcasted_iota(jnp.int32, (BLOCK, 2 * BLOCK), 0)
        j = lax.broadcasted_iota(jnp.int32, (BLOCK, 2 * BLOCK), 1) - BLOCK
        for g, window in enumerate((2 + 6 * t, 4 + 12 * t)):
            band[g] = jnp.where((j <= i) & (j > i - window), 1.0, 0.0).astype(BF16)

    def mean_inverse(total):
        return lax.rsqrt(total * (1.0 / (2 * HALF)) + EPS)

    def row_sum(v):
        return jnp.sum(v, axis=1, keepdims=True)

    SUB = 16

    def first_norm(i):
        loads[i].wait()
        arrived(0, i, x_buf.at[other, rows_of(i)])
        g0, g1 = gains[0:1, 0:HALF], gains[0:1, HALF:]

        def body(k, _):
            rows = pl.ds(pl.multiple_of(i * BLOCK + k * SUB, SUB), SUB)
            a, b = x_buf[0, rows].astype(F32), x_buf[1, rows].astype(F32)
            inverse = mean_inverse(row_sum(a * a + b * b))
            normed[rows, 0:HALF] = (a * inverse * g0).astype(BF16)
            normed[rows, HALF:] = (b * inverse * g1).astype(BF16)
            return 0

        lax.fori_loop(0, BLOCK // SUB, body, 0, unroll=2)

    def mix(c):
        cols = slice(256 * c, 256 * c + 256)
        weight = w0[:, :, :, 0:64, cols].reshape(2 * HALF, 256)

        def body(i, _):
            rows = pl.ds(pl.multiple_of(i * MROWS, MROWS), MROWS)
            mixed[rows, cols] = (dot(normed[rows], weight) * scale[0:1, cols]).astype(BF16)
            return 0

        lax.fori_loop(0, LENGTH // MROWS, body, 0)

    def pool(i):
        rows = slice(i * BLOCK, i * BLOCK + BLOCK)
        for g in range(2):
            cols = slice(GW * g, GW * g + GW)
            window = (2 + 6 * t, 4 + 12 * t)[g]
            own = mixed[rows, cols]
            if i == 0:
                sums = dot(band[g, :, BLOCK:], own)
                position = lax.broadcasted_iota(jnp.int32, (BLOCK, 1), 0)
                sums = sums / jnp.minimum(position + 1, window).astype(F32)
            else:
                sums = dot(band[g], mixed[rows.start - BLOCK : rows.stop, cols])
                sums = sums * (1.0 / jnp.full((BLOCK, 1), window, jnp.int32).astype(F32))
            pooled = (sums - own.astype(F32)).astype(BF16)
            weight = w0[:, :, :, 64:80, cols].reshape(GW, GW)
            branch[t, rows, cols] = (dot(pooled, weight) * scale[1:2, cols]).astype(BF16)

    def branch_share(i):
        share(1, i, branch.at[t, rows_of(i)], branch.at[t, rows_of(i)])

    def middle(i):
        arrived(1, i, branch.at[other, rows_of(i)])
        post = [gains[1:2, 0:HALF], gains[1:2, HALF:]]
        pre = [gains[2:3, 0:HALF], gains[2:3, HALF:]]

        def body(k, _):
            rows = pl.ds(pl.multiple_of(i * BLOCK + k * SUB, SUB), SUB)
            parts = [branch[h, rows].astype(F32) for h in range(2)]
            inverse = mean_inverse(row_sum(parts[0] * parts[0] + parts[1] * parts[1]))
            mids = []
            for h in range(2):
                add = (parts[h] * inverse * post[h]).astype(BF16).astype(F32)
                mid = (x_buf[h, rows].astype(F32) + add).astype(BF16)
                x_buf[h, rows] = mid
                mids.append(mid.astype(F32))
            inverse = mean_inverse(row_sum(mids[0] * mids[0] + mids[1] * mids[1]))
            for h in range(2):
                normed[rows, h * HALF : h * HALF + HALF] = (mids[h] * inverse * pre[h]).astype(BF16)
            return 0

        lax.fori_loop(0, BLOCK // SUB, body, 0, unroll=2)

    def up(b, c):
        cols = slice(256 * c, 256 * c + 256)
        place = slice((b - 1) * 1024 + 256 * c, (b - 1) * 1024 + 256 * c + 256)
        weight = bufs[b][:, :, :, :, cols].reshape(2 * HALF, 256)

        def body(i, _):
            rows = pl.ds(pl.multiple_of(i * MROWS, MROWS), MROWS)
            act = jnp.maximum(dot(normed[rows], weight) * scale[b + 1 : b + 2, cols], 0.0)
            hidden[rows, place] = (act * act).astype(BF16)
            return 0

        lax.fori_loop(0, LENGTH // MROWS, body, 0)

    def down(b, n, part=None):
        buf, lane, width = BATCHES[b]
        half, k = (other, n) if n < 2 else (t, n - 2)
        first = (buf - 3) * 1024 + lane
        weight = bufs[buf][half, 2 * k : 2 * k + 2, :, :, lane : lane + 4 * width]
        weight = weight.reshape(512, 4 * width)
        cols = slice(512 * k, 512 * k + 512)

        def body(i, _):
            rows = pl.ds(pl.multiple_of(i * MROWS, MROWS), MROWS)
            value = dot_t(hidden[rows, first : first + 4 * width], weight)
            if b > 3:
                value = value + acc[half, rows, cols]
            if b < NB - 1:
                acc[half, rows, cols] = value
            elif n < 2:
                part_out[rows, cols] = value.astype(BF16)
            else:
                mixed[rows, cols] = value.astype(BF16)
            return 0

        if part is not None:
            body(part, 0)
        else:
            lax.fori_loop(0, LENGTH // MROWS, body, 0)

    def last(part):
        for n in range(2):
            down(NB - 1, n, part)
        share(2, part, part_out.at[rows_of(part, 512)], part_in.at[rows_of(part, 512)])

    def last_own(part):
        for n in range(2, 4):
            down(NB - 1, n, part)

    def total(i):
        if i % 2 == 0:
            arrived(2, i // 2, part_in.at[rows_of(i // 2, 512)])

        def body(k, _):
            rows = pl.ds(pl.multiple_of(i * BLOCK + k * SUB, SUB), SUB)
            both = mixed[rows].astype(F32) + part_in[rows].astype(F32)
            value = (both * scale[4:5]).astype(BF16)
            mixed[rows] = value
            value = value.astype(F32)
            square = value * value
            lanes = square[:, 0:128]
            for q in range(1, 8):
                lanes = lanes + square[:, 128 * q : 128 * q + 128]
            squares[t, rows] = lanes
            return 0

        lax.fori_loop(0, BLOCK // SUB, body, 0, unroll=2)
        share(3, i, squares.at[t, rows_of(i)], squares.at[t, rows_of(i)])

    def final(i):
        arrived(3, i, squares.at[other, rows_of(i)])
        gain = gains[3:4, pl.ds(pl.multiple_of(t * HALF, HALF), HALF)]
        squared = squares[0, rows_of(i)] + squares[1, rows_of(i)]
        inverses[...] = jnp.broadcast_to(mean_inverse(row_sum(squared)), (BLOCK, 128))

        def body(k, _):
            at = pl.ds(pl.multiple_of(k * SUB, SUB), SUB)
            rows = pl.ds(pl.multiple_of(i * BLOCK + k * SUB, SUB), SUB)
            inverse = jnp.concatenate([inverses[at]] * (HALF // 128), axis=1)
            add = (mixed[rows].astype(F32) * inverse * gain).astype(BF16).astype(F32)
            mixed[rows] = (x_buf[t, rows].astype(F32) + add).astype(BF16)
            return 0

        lax.fori_loop(0, BLOCK // SUB, body, 0, unroll=2)
        copy = pltpu.make_async_copy(mixed.at[rows_of(i)], out.at[rows_of(i)], out_sem.at[i])
        copy.start()
        outs.append(copy)

    def run(name, step, *args):
        with jax.named_scope(name):
            step(*args)

    steps = dict(
        sc=scales, bands=bands, norm=first_norm, mix=mix, pool=pool, mid=middle, up=up, dn=down
    )
    steps.update(T=gather.tick, share=branch_share, total=total, final=final)
    steps.update(last=last, own=last_own)
    run("sc", scales, 0)
    for name, *args in PLAN:
        run("#".join(map(str, (name, *args))), steps[name], *args)
    with jax.named_scope("finish"):
        gather.finish()
        for copy in sent:
            copy.wait_send()
    with jax.named_scope("outs"):
        for copy in outs:
            copy.wait()


def on_device(
    tokens,
    norm_gains,
    mix_weight,
    mix_scale,
    group_weight,
    group_scale,
    up_weight,
    up_scale,
    down_weight,
    down_scale,
):
    arrays = (tokens, norm_gains, mix_weight, group_weight, up_weight, down_weight.T)
    arrays += (mix_scale.T, group_scale.T, up_scale.T, down_scale.T)
    dma = pltpu.SemaphoreType.DMA
    return pl.pallas_call(
        kernel,
        out_shape=jax.ShapeDtypeStruct((LENGTH, HALF), BF16),
        in_specs=[pl.BlockSpec(memory_space=pl.ANY)] + [pl.BlockSpec(memory_space=pl.ANY)] * 9,
        out_specs=pl.BlockSpec(memory_space=pl.ANY),
        scratch_shapes=[pltpu.VMEM(a.shape, F32) for a in arrays[1:]]
        + [pltpu.VMEM((2, 4, 4, r, 1024), BF16) for r in ROWS]
        + [
            pltpu.VMEM((2, LENGTH, HALF), BF16),
            pltpu.VMEM((LENGTH, 2 * HALF), BF16),
            pltpu.VMEM((LENGTH, HALF), BF16),
            pltpu.VMEM((2, LENGTH, HALF), BF16),
            pltpu.VMEM((LENGTH, 2048), BF16),
            pltpu.VMEM((2, LENGTH, HALF), F32),
            pltpu.VMEM((LENGTH, HALF), BF16),
            pltpu.VMEM((LENGTH, HALF), BF16),
            pltpu.VMEM((2, LENGTH, 128), F32),
            pltpu.VMEM((2, BLOCK, 2 * BLOCK), BF16),
            pltpu.VMEM((40, 128), F32),
            pltpu.VMEM((7, 40, 128), F32),
            pltpu.VMEM((2, 40, 128), F32),
            pltpu.VMEM((5, 1024), F32),
            pltpu.VMEM((BLOCK, 128), F32),
            dma((POOL,)),
            dma((NB, 4, 5)),
            dma((9 + NR,)),
            dma((4, NR)),
            dma((4, NR)),
            dma((7,)),
            dma((7,)),
            dma((NR,)),
        ],
        compiler_params=pltpu.CompilerParams(
            collective_id=0, has_side_effects=True, vmem_limit_bytes=67_000_000
        ),
    )(*arrays)


def solution(mesh):
    finer = Mesh(
        mesh.devices.reshape(mesh.shape["rep"], 2, 4, 4, mesh.shape["tp"]),
        ("rep", "fs_0", "fs_1", "fs_2", "tp"),
    )
    in_specs = (
        P(REP_FS, "tp"),
        P(),
        P(FS, "tp"),
        P("tp", FS),
        P("tp", FS, None),
        P("tp", FS),
        P(FS, "tp"),
        P("tp", FS),
        P("tp", FS),
        P("tp", FS),
    )
    out_specs = P(REP_FS, "tp")
    return jax.shard_map(
        on_device, mesh=finer, in_specs=in_specs, out_specs=out_specs, check_vma=False
    )
```

```python
import functools

import jax
import jax.numpy as jnp
from jax import lax
from jax.experimental import pallas as pl
from jax.experimental.pallas import tpu as pltpu
from jax.sharding import Mesh
from jax.sharding import PartitionSpec as P

FS = ("fs_0", "fs_1", "fs_2")
REP_FS = ("rep", "fs_0", "fs_1", "fs_2")
MESH = pl.DeviceIdType.MESH
ALL = slice(None)
EPS = 1e-06

LENGTH = 1024
HALF = 1024
GW = 512
ROWS = (80, 64, 64, 64, 64)
BATCHES = (
    (0, 0, 64, 0, 256),
    (0, 64, 16, 0, 256),
    (1, 0, 64, 0, 256),
    (2, 0, 64, 0, 256),
    (3, 0, 64, 0, 256),
    (4, 0, 64, 0, 128),
    (4, 0, 64, 512, 128),
)
NB = len(BATCHES)
POOL = 44
LAG = 10
MROWS = 512
BLOCK = 256
NR = LENGTH // BLOCK
F32, BF16 = jnp.float32, jnp.bfloat16


PLAN = (
    ("T", 1, 0, 0), ("T", 1, 1, 0), ("T", 3, 0, 0), ("T", 2, 0, 0), ("T", 3, 1, 0), ("T", 2, 1, 0),
    ("T", 4, 0, 0), ("bands",), ("T", 4, 1, 0), ("T", 5, 0, 0), ("T", 5, 1, 0), ("T", 6, 0, 0),
    ("T", 6, 1, 0), ("T", 0, 0, 1), ("sc", 1), ("sc", 2), ("T", 0, 1, 1), ("norm", 0), ("T", 1, 0, 1),
    ("T", 1, 1, 1), ("norm", 1), ("T", 3, 0, 1), ("T", 2, 0, 1), ("norm", 2), ("T", 3, 1, 1), ("norm", 3),
    ("T", 2, 1, 1), ("T", 4, 0, 1), ("sc", 3), ("T", 4, 1, 1), ("sc", 4), ("T", 5, 0, 1), ("T", 5, 1, 1),
    ("T", 6, 0, 1), ("T", 6, 1, 1), ("T", 0, 0, 2), ("T", 0, 1, 2), ("T", 1, 0, 2), ("T", 1, 1, 2),
    ("T", 3, 0, 2), ("T", 3, 1, 2), ("T", 2, 0, 2), ("sc", 5), ("T", 4, 1, 2), ("T", 4, 0, 2),
    ("T", 5, 1, 2), ("T", 0, 0, 3), ("T", 0, 1, 3), ("T", 6, 0, 2), ("T", 1, 0, 3), ("T", 1, 1, 3),
    ("T", 6, 1, 2), ("T", 2, 1, 2), ("T", 0, 0, 4), ("T", 5, 0, 2), ("T", 4, 0, 3), ("T", 4, 1, 3),
    ("T", 0, 1, 4), ("T", 2, 0, 3), ("T", 2, 1, 3), ("T", 1, 0, 4), ("T", 1, 1, 4), ("T", 3, 0, 3),
    ("T", 3, 1, 3), ("T", 4, 0, 4), ("T", 0, 0, 5), ("mix", 0), ("T", 0, 1, 5), ("mix", 1), ("T", 2, 0, 4),
    ("T", 2, 1, 4), ("T", 4, 1, 4), ("T", 1, 0, 5), ("T", 1, 1, 5), ("pool", 0), ("share", 0), ("pool", 1),
    ("T", 3, 0, 4), ("share", 1), ("pool", 2), ("share", 2), ("pool", 3), ("share", 3), ("mid", 0),
    ("T", 6, 0, 3), ("mid", 1), ("mid", 2), ("T", 5, 0, 3), ("T", 3, 1, 4), ("T", 5, 1, 3), ("T", 6, 1, 3),
    ("mid", 3), ("T", 2, 0, 5), ("up", 1, 0), ("T", 2, 1, 5), ("up", 1, 1), ("T", 6, 0, 4), ("T", 4, 0, 5),
    ("T", 4, 1, 5), ("dn", 4, 0), ("T", 5, 0, 4), ("dn", 4, 1), ("dn", 4, 2), ("T", 3, 1, 5), ("up", 2, 1),
    ("T", 5, 1, 4), ("T", 3, 0, 5), ("up", 2, 0), ("T", 6, 1, 4), ("dn", 4, 3), ("T", 5, 0, 5),
    ("T", 5, 1, 5), ("dn", 5, 0), ("dn", 5, 1), ("dn", 5, 2), ("dn", 5, 3), ("T", 6, 0, 5), ("T", 6, 1, 5),
    ("last", 0), ("last", 1), ("own", 0), ("total", 0), ("total", 1), ("own", 1), ("total", 2),
    ("total", 3), ("final", 0), ("final", 1), ("final", 2), ("final", 3),
)
ORDERS = (
    ("xyz", "xzy"),
    ("xzy", "xzy"),
    ("xyz", "xzy"),
    ("xyz", "xzy"),
    ("xyz", "xzy"),
    ("xyz", "xzy"),
    ("xzy", "xzy"),
)


def dot(a, b):
    return jnp.dot(a, b, preferred_element_type=F32)


def dot_t(a, b):
    return lax.dot_general(a, b, (((1,), (1,)), ((), ())), preferred_element_type=F32)


def spot():
    return dict(
        z=lax.axis_index("rep") * 2 + lax.axis_index("fs_0"),
        y=lax.axis_index("fs_1"),
        x=lax.axis_index("fs_2"),
        t=lax.axis_index("tp"),
    )


def to(axis, at):
    if axis == "x":
        return {"fs_2": at}
    if axis == "y":
        return {"fs_1": at}
    if axis == "z":
        return {"rep": at // 2, "fs_0": at % 2}
    return {"tp": at}


def send(src, dst, send_sem, recv_sem, axis, at):
    return pltpu.make_async_remote_copy(
        src_ref=src,
        dst_ref=dst,
        send_sem=send_sem,
        recv_sem=recv_sem,
        device_id=to(axis, at),
        device_id_type=MESH,
    )


class Gather:
    def __init__(self, bufs, send_sem, recv_sem, me):
        self.bufs, self.send_sem, self.recv_sem, self.me = bufs, send_sem, recv_sem, me
        self.sent, self.ticks, self.free = [], 0, list(range(POOL))
        self.steps = {
            (b, p): self.plan(b, p, order) for b in range(NB) for p, order in enumerate(ORDERS[b])
        }

    def region(self, b, c, at, half=None, colours=1):
        buf, row, rows, lane, width = BATCHES[b]
        lane, width = lane + width * c, width * colours
        if half is not None and width == 256:
            lane, width = lane + 128 * half, 128
        elif half is not None:
            row, rows = row + rows // 2 * half, rows // 2
        return self.bufs[buf].at[at["z"], at["y"], at["x"], pl.ds(row, rows), pl.ds(lane, width)]

    def plan(self, b, p, order):
        me = self.me
        owns = [dict(z=me["z"] % 2, y=me["y"], x=me["x"])] * 2
        steps = []
        for axis in order:
            if axis == "z":
                copies = []
                for k, d in enumerate((1, 3)):
                    ref = self.region(b, 2 * p + k, owns[k])
                    copies.append((ref, "z", lax.rem(me["z"] + d, 4)))
                steps.append((copies, self.region(b, 2 * p, owns[0], colours=2)))
            else:
                first, second = [], []
                for k in range(2):
                    along = axis if k == 0 else {"x": "y", "y": "x"}[axis]
                    up, down = lax.rem(me[along] + 1, 4), lax.rem(me[along] + 3, 4)

                    def part(i, half=None):
                        return self.region(b, 2 * p + k, {**owns[k], along: i}, half)

                    first += [(part(me[along]), along, up), (part(me[along]), along, down)]
                    second += [(part(down, 0), along, up), (part(up, 1), along, down)]
                two = self.region(b, 2 * p, {**owns[0], axis: pl.ds(0, 2)}, colours=2)
                steps.append((first, two))
                steps.append((second, self.region(b, 2 * p, owns[0], colours=2)))
            owns = [{**own, axis if k == 0 else {"x": "y", "y": "x", "z": "z"}[axis]: ALL} for k, own in enumerate(owns)]
        return steps

    def copy(self, b, p, k, pool, ref, axis, at):
        return send(ref, ref, self.send_sem.at[pool], self.recv_sem.at[b, p, k], axis, at)

    def tick(self, b, p, s):
        self.ticks += 1
        while self.sent and self.sent[0][0] < self.ticks - LAG:
            self.release()
        if s > 0:
            ref = self.steps[b, p][s - 1][1]
            self.copy(b, p, s - 1, 0, ref, "x", self.me["x"]).wait_recv()
        if s < 5:
            for ref, axis, at in self.steps[b, p][s][0]:
                if not self.free:
                    self.release()
                pool = self.free.pop(0)
                copy = self.copy(b, p, s, pool, ref, axis, at)
                copy.start()
                self.sent.append((self.ticks, pool, copy))

    def release(self):
        _, pool, copy = self.sent.pop(0)
        copy.wait_send()
        self.free.append(pool)

    def finish(self):
        while self.sent:
            self.release()


def greet(me, wait):
    barrier = pltpu.get_barrier_semaphore()
    peers = [("x", 1), ("x", 2), ("x", 3), ("y", 1), ("y", 2), ("y", 3), ("z", 1), ("z", 3)]
    if wait:
        pl.semaphore_wait(barrier, len(peers) + 1)
        return
    for axis, d in peers:
        pl.semaphore_signal(
            barrier, inc=1, device_id=to(axis, lax.rem(me[axis] + d, 4)), device_id_type=MESH
        )
    pl.semaphore_signal(barrier, inc=1, device_id=to("t", 1 - me["t"]), device_id_type=MESH)


def kernel(
    tokens,
    gains_in,
    mix_in,
    group_in,
    up_in,
    down_in,
    mix_s_in,
    group_s_in,
    up_s_in,
    down_s_in,
    out,
    gains,
    mix_w,
    group_w,
    up_w,
    down_w,
    mix_s,
    group_s,
    up_s,
    down_s,
    w0,
    w1,
    w2,
    w3,
    w4,
    x_buf,
    normed,
    mixed,
    branch,
    hidden,
    acc,
    part_out,
    part_in,
    squares,
    band,
    tile,
    sc_in,
    sc_sum,
    scale,
    inverses,
    g_send,
    g_recv,
    load_sem,
    p_send,
    p_recv,
    s_send,
    s_recv,
):
    me = spot()
    greet(me, False)
    t, other = me["t"], 1 - me["t"]
    here = (me["z"] % 2, me["y"], me["x"])
    bufs = (w0, w1, w2, w3, w4)
    gather = Gather(bufs, g_send, g_recv, me)
    sent = []

    def rows_of(i, size=BLOCK):
        return pl.ds(i * size, size)

    def scale_tile():
        place = me["z"] % 2 * 16 + me["y"] * 4 + me["x"]
        lane = lax.broadcasted_iota(jnp.int32, (1, 128), 1)
        base = 0
        for ref in (mix_s, group_s, up_s, down_s):
            n = ref.shape[1] // 2
            q = lax.broadcasted_iota(jnp.int32, (n, 2 * n), 0)
            r = lax.broadcasted_iota(jnp.int32, (n, 2 * n), 1)
            value = jnp.zeros((n, 128), F32)
            for j in range(2):
                for h in range(2):
                    own = jnp.where(r == 2 * q + h, ref[j : j + 1], 0.0)
                    column = jnp.sum(own, axis=1, keepdims=True)
                    value = value + jnp.where(lane == h * 64 + 2 * place + j, column, 0.0)
            tile[base : base + n] = value
            base += n

    def load(k, src, dst):
        copy = pltpu.make_async_copy(src, dst, load_sem.at[k])
        copy.start()
        return copy

    pairs = (
        (mix_in, mix_w),
        (group_in, group_w),
        (mix_s_in, mix_s),
        (group_s_in, group_s),
        (up_s_in, up_s),
        (down_s_in, down_s),
        (up_in, up_w),
        (down_in, down_w),
        (gains_in, gains),
    )
    early = [load(k, src, dst) for k, (src, dst) in enumerate(pairs)]
    loads = [
        load(len(pairs) + i, tokens.at[rows_of(i)], x_buf.at[t, rows_of(i)]) for i in range(NR)
    ]
    for copy in early[:6]:
        copy.wait()
    w0[here[0], here[1], here[2], 0:64] = mix_w[...].astype(BF16)
    w0[here[0], here[1], here[2], 64:80, 0:GW] = group_w[0].astype(BF16)
    w0[here[0], here[1], here[2], 64:80, GW:] = group_w[1].astype(BF16)
    scale_tile()
    for copy in early[6:]:
        copy.wait()
    up_all, down_all = up_w[...].astype(BF16), down_w[...].astype(BF16)
    for ref, lane in ((w1, 0), (w2, 1024)):
        ref[here[0], here[1], here[2]] = up_all[:, lane : lane + 1024]
    for ref, lane in ((w3, 0), (w4, 1024)):
        ref[here[0], here[1], here[2]] = down_all[:, lane : lane + 1024]
    with jax.named_scope("greet"):
        greet(me, True)

    def share(kind, i, src, dst):
        copy = send(src, dst, p_send.at[kind, i], p_recv.at[kind, i], "t", other)
        copy.start()
        sent.append(copy)

    def arrived(kind, i, ref):
        send(ref, ref, p_send.at[kind, i], p_recv.at[kind, i], "t", other).wait_recv()

    for p in range(2):
        gather.tick(0, p, 0)
    for i in range(NR):
        share(0, i, tokens.at[rows_of(i)], x_buf.at[t, rows_of(i)])

    def scale_send(slot, src, axis, at):
        copy = send(src, sc_in.at[slot], s_send.at[slot], s_recv.at[slot], axis, at)
        copy.start()
        sent.append(copy)

    def scale_wait(slot):
        send(sc_in.at[slot], sc_in.at[slot], s_send.at[slot], s_recv.at[slot], "t", other).wait_recv()

    def scales(step):
        if step == 0:
            for d in (1, 2, 3):
                scale_send(d - 1, tile, "x", lax.rem(me["x"] + d, 4))
        if step == 1:
            for d in (1, 2, 3):
                scale_wait(d - 1)
            sc_sum[0] = tile[...] + sc_in[0] + sc_in[1] + sc_in[2]
        if step == 2:
            for d in (1, 2, 3):
                scale_send(d + 2, sc_sum.at[0], "y", lax.rem(me["y"] + d, 4))
        if step == 3:
            for d in (1, 2, 3):
                scale_wait(d + 2)
            sc_sum[1] = sc_sum[0] + sc_in[3] + sc_in[4] + sc_in[5]
        if step == 4:
            scale_send(6, sc_sum.at[1], "z", me["z"] + 1 - 2 * (me["z"] % 2))
        if step == 5:
            scale_wait(6)
            whole = sc_sum[1] + sc_in[6]
            for q in range(40):
                scale[q // 8 : q // 8 + 1, 128 * (q % 8) : 128 * (q % 8) + 128] = whole[q : q + 1]

    def bands():
        i = lax.broadcasted_iota(jnp.int32, (BLOCK, 2 * BLOCK), 0)
        j = lax.broadcasted_iota(jnp.int32, (BLOCK, 2 * BLOCK), 1) - BLOCK
        for g, window in enumerate((2 + 6 * t, 4 + 12 * t)):
            band[g] = jnp.where((j <= i) & (j > i - window), 1.0, 0.0).astype(BF16)

    def mean_inverse(total):
        return lax.rsqrt(total * (1.0 / (2 * HALF)) + EPS)

    def row_sum(v):
        return jnp.sum(v, axis=1, keepdims=True)

    SUB, UNROLL = 16, 4

    def first_norm(i):
        loads[i].wait()
        arrived(0, i, x_buf.at[other, rows_of(i)])
        g0, g1 = gains[0:1, 0:HALF], gains[0:1, HALF:]

        def body(k, _):
            rows = pl.ds(pl.multiple_of(i * BLOCK + k * SUB, SUB), SUB)
            a, b = x_buf[0, rows].astype(F32), x_buf[1, rows].astype(F32)
            inverse = mean_inverse(row_sum(a * a + b * b))
            normed[rows, 0:HALF] = (a * inverse * g0).astype(BF16)
            normed[rows, HALF:] = (b * inverse * g1).astype(BF16)
            return 0

        lax.fori_loop(0, BLOCK // SUB, body, 0, unroll=UNROLL)

    def mix(p):
        cols = slice(GW * p, GW * p + GW)
        weight = w0[:, :, :, 0:64, cols].reshape(2 * HALF, GW)
        mixed[:, cols] = (dot(normed[...], weight) * scale[0:1, cols]).astype(BF16)

    def pool(i):
        rows = slice(i * BLOCK, i * BLOCK + BLOCK)
        for g in range(2):
            cols = slice(GW * g, GW * g + GW)
            window = (2 + 6 * t, 4 + 12 * t)[g]
            own = mixed[rows, cols]
            if i == 0:
                sums = dot(band[g, :, BLOCK:], own)
                position = lax.broadcasted_iota(jnp.int32, (BLOCK, 1), 0)
                sums = sums / jnp.minimum(position + 1, window).astype(F32)
            else:
                sums = dot(band[g], mixed[rows.start - BLOCK : rows.stop, cols])
                sums = sums * (1.0 / jnp.full((BLOCK, 1), window, jnp.int32).astype(F32))
            pooled = (sums - own.astype(F32)).astype(BF16)
            weight = w0[:, :, :, 64:80, cols].reshape(GW, GW)
            branch[t, rows, cols] = (dot(pooled, weight) * scale[1:2, cols]).astype(BF16)

    def branch_share(i):
        share(1, i, branch.at[t, rows_of(i)], branch.at[t, rows_of(i)])

    def middle(i):
        arrived(1, i, branch.at[other, rows_of(i)])
        post = [gains[1:2, 0:HALF], gains[1:2, HALF:]]
        pre = [gains[2:3, 0:HALF], gains[2:3, HALF:]]

        def body(k, _):
            rows = pl.ds(pl.multiple_of(i * BLOCK + k * SUB, SUB), SUB)
            parts = [branch[h, rows].astype(F32) for h in range(2)]
            inverse = mean_inverse(row_sum(parts[0] * parts[0] + parts[1] * parts[1]))
            mids = []
            for h in range(2):
                add = (parts[h] * inverse * post[h]).astype(BF16).astype(F32)
                mid = (x_buf[h, rows].astype(F32) + add).astype(BF16)
                x_buf[h, rows] = mid
                mids.append(mid.astype(F32))
            inverse = mean_inverse(row_sum(mids[0] * mids[0] + mids[1] * mids[1]))
            for h in range(2):
                normed[rows, h * HALF : h * HALF + HALF] = (mids[h] * inverse * pre[h]).astype(BF16)
            return 0

        lax.fori_loop(0, BLOCK // SUB, body, 0, unroll=UNROLL)

    def up(buf, p):
        cols = slice(512 * p, 512 * p + 512)
        place = slice((buf - 1) * 1024 + 512 * p, (buf - 1) * 1024 + 512 * p + 512)
        weight = bufs[buf][:, :, :, :, cols].reshape(2 * HALF, 512)
        act = jnp.maximum(dot(normed[...], weight) * scale[buf + 1 : buf + 2, cols], 0.0)
        hidden[:, place] = (act * act).astype(BF16)

    def down(b, n, part=None):
        buf, _, _, lane, width = BATCHES[b]
        half, k = (other, n) if n < 2 else (t, n - 2)
        first = (buf - 3) * 1024 + lane
        weight = bufs[buf][half, 2 * k : 2 * k + 2, :, :, lane : lane + 4 * width]
        weight = weight.reshape(512, 4 * width)
        cols = slice(512 * k, 512 * k + 512)

        def body(i, _):
            rows = pl.ds(pl.multiple_of(i * MROWS, MROWS), MROWS)
            value = dot_t(hidden[rows, first : first + 4 * width], weight)
            if buf > 3:
                value = value + acc[half, rows, cols]
            if b < NB - 1:
                acc[half, rows, cols] = value
            elif n < 2:
                part_out[rows, cols] = value.astype(BF16)
            else:
                mixed[rows, cols] = value.astype(BF16)
            return 0

        if part is not None:
            body(part, 0)
        else:
            lax.fori_loop(0, LENGTH // MROWS, body, 0)

    def last(part):
        for n in range(2):
            down(NB - 1, n, part)
        share(2, part, part_out.at[rows_of(part, 512)], part_in.at[rows_of(part, 512)])

    def last_own(part):
        for n in range(2, 4):
            down(NB - 1, n, part)

    def total(i):
        if i % 2 == 0:
            arrived(2, i // 2, part_in.at[rows_of(i // 2, 512)])

        def body(k, _):
            rows = pl.ds(pl.multiple_of(i * BLOCK + k * SUB, SUB), SUB)
            both = mixed[rows].astype(F32) + part_in[rows].astype(F32)
            value = (both * scale[4:5]).astype(BF16)
            mixed[rows] = value
            value = value.astype(F32)
            square = value * value
            lanes = square[:, 0:128]
            for q in range(1, 8):
                lanes = lanes + square[:, 128 * q : 128 * q + 128]
            squares[t, rows] = lanes
            return 0

        lax.fori_loop(0, BLOCK // SUB, body, 0, unroll=UNROLL)
        share(3, i, squares.at[t, rows_of(i)], squares.at[t, rows_of(i)])

    def final(i):
        arrived(3, i, squares.at[other, rows_of(i)])
        gain = gains[3:4, pl.ds(pl.multiple_of(t * HALF, HALF), HALF)]
        squared = squares[0, rows_of(i)] + squares[1, rows_of(i)]
        inverses[...] = jnp.broadcast_to(mean_inverse(row_sum(squared)), (BLOCK, 128))

        def body(k, _):
            at = pl.ds(pl.multiple_of(k * SUB, SUB), SUB)
            rows = pl.ds(pl.multiple_of(i * BLOCK + k * SUB, SUB), SUB)
            inverse = jnp.concatenate([inverses[at]] * (HALF // 128), axis=1)
            add = (mixed[rows].astype(F32) * inverse * gain).astype(BF16).astype(F32)
            out[rows] = (x_buf[t, rows].astype(F32) + add).astype(BF16)
            return 0

        lax.fori_loop(0, BLOCK // SUB, body, 0, unroll=UNROLL)

    def run(name, step, *args):
        with jax.named_scope(name):
            step(*args)

    steps = dict(
        sc=scales, bands=bands, norm=first_norm, mix=mix, pool=pool, mid=middle, up=up, dn=down
    )
    steps.update(T=gather.tick, share=branch_share, total=total, final=final)
    steps.update(last=last, own=last_own)
    run("sc", scales, 0)
    for name, *args in PLAN:
        run("#".join(map(str, (name, *args))), steps[name], *args)
    with jax.named_scope("finish"):
        gather.finish()
        for copy in sent:
            copy.wait_send()


def on_device(
    tokens,
    norm_gains,
    mix_weight,
    mix_scale,
    group_weight,
    group_scale,
    up_weight,
    up_scale,
    down_weight,
    down_scale,
):
    arrays = (tokens, norm_gains, mix_weight, group_weight, up_weight, down_weight.T)
    arrays += (mix_scale.T, group_scale.T, up_scale.T, down_scale.T)
    dma = pltpu.SemaphoreType.DMA
    return pl.pallas_call(
        kernel,
        out_shape=pltpu.VMEM((LENGTH, HALF), BF16),
        in_specs=[pl.BlockSpec(memory_space=pl.ANY)] + [pl.BlockSpec(memory_space=pl.ANY)] * 9,
        out_specs=pl.BlockSpec(memory_space=pltpu.VMEM),
        scratch_shapes=[pltpu.VMEM(a.shape, F32) for a in arrays[1:]]
        + [pltpu.VMEM((2, 4, 4, r, 1024), BF16) for r in ROWS]
        + [
            pltpu.VMEM((2, LENGTH, HALF), BF16),
            pltpu.VMEM((LENGTH, 2 * HALF), BF16),
            pltpu.VMEM((LENGTH, HALF), BF16),
            pltpu.VMEM((2, LENGTH, HALF), BF16),
            pltpu.VMEM((LENGTH, 2048), BF16),
            pltpu.VMEM((2, LENGTH, HALF), F32),
            pltpu.VMEM((LENGTH, HALF), BF16),
            pltpu.VMEM((LENGTH, HALF), BF16),
            pltpu.VMEM((2, LENGTH, 128), F32),
            pltpu.VMEM((2, BLOCK, 2 * BLOCK), BF16),
            pltpu.VMEM((40, 128), F32),
            pltpu.VMEM((7, 40, 128), F32),
            pltpu.VMEM((2, 40, 128), F32),
            pltpu.VMEM((5, 1024), F32),
            pltpu.VMEM((BLOCK, 128), F32),
            dma((POOL,)),
            dma((NB, 2, 5)),
            dma((9 + NR,)),
            dma((4, NR)),
            dma((4, NR)),
            dma((7,)),
            dma((7,)),
        ],
        compiler_params=pltpu.CompilerParams(
            collective_id=0, has_side_effects=True, vmem_limit_bytes=60_000_000
        ),
    )(*arrays)


def solution(mesh):
    finer = Mesh(
        mesh.devices.reshape(mesh.shape["rep"], 2, 4, 4, mesh.shape["tp"]),
        ("rep", "fs_0", "fs_1", "fs_2", "tp"),
    )
    in_specs = (
        P(REP_FS, "tp"),
        P(),
        P(FS, "tp"),
        P("tp", FS),
        P("tp", FS, None),
        P("tp", FS),
        P(FS, "tp"),
        P("tp", FS),
        P("tp", FS),
        P("tp", FS),
    )
    out_specs = P(REP_FS, "tp")
    return jax.shard_map(
        on_device, mesh=finer, in_specs=in_specs, out_specs=out_specs, check_vma=False
    )
```

```python
import functools

import jax
import jax.numpy as jnp
from jax import lax
from jax.experimental import pallas as pl
from jax.experimental.pallas import tpu as pltpu
from jax.sharding import Mesh
from jax.sharding import PartitionSpec as P

FS = ("fs_0", "fs_1", "fs_2")
REP_FS = ("rep", "fs_0", "fs_1", "fs_2")
MESH = pl.DeviceIdType.MESH
ALL = slice(None)
EPS = 1e-06

LENGTH = 1024
HALF = 1024
GW = 512
ROWS = (80, 64, 64, 64, 64)
KCUT = 512
BATCHES = (
    (0, 0, 64, 0, 256, 0, 256),
    (0, 64, 16, 0, 256, 0, 256),
    (1, 0, 64, 0, 256, 0, 256),
    (2, 0, 64, 0, 256, 0, 256),
    (3, 0, 64, 0, 256, 0, 256),
    (4, 0, 16, 0, KCUT, 16, 0),
    (4, 0, 16, KCUT, 1024 - KCUT, 16, 0),
)
NB = len(BATCHES)
POOL = 54
MROWS = 512
BLOCK = 256
NR = LENGTH // BLOCK
F32, BF16 = jnp.float32, jnp.bfloat16


PLAN = (
    ("T", 1, 1, 0), ("T", 1, 0, 0), ("T", 3, 0, 0), ("T", 2, 1, 0), ("T", 5, 0, 0), ("T", 6, 0, 0),
    ("T", 4, 1, 0), ("T", 2, 0, 0), ("T", 0, 1, 1), ("T", 0, 0, 1), ("sc", 1), ("T", 3, 1, 0),
    ("T", 4, 0, 0), ("T", 1, 0, 1), ("T", 5, 0, 1), ("T", 3, 0, 1), ("T", 2, 1, 1), ("T", 6, 1, 0),
    ("sc", 2), ("T", 2, 0, 1), ("T", 0, 1, 2), ("T", 1, 1, 1), ("T", 4, 1, 1), ("bands",), ("T", 0, 0, 2),
    ("T", 1, 0, 2), ("norm", 0), ("T", 5, 0, 2), ("norm", 1), ("T", 2, 1, 2), ("norm", 3), ("T", 3, 1, 1),
    ("T", 1, 1, 2), ("T", 6, 0, 1), ("T", 2, 0, 2), ("T", 0, 0, 3), ("T", 4, 1, 2), ("T", 3, 1, 2),
    ("T", 5, 1, 0), ("T", 1, 0, 3), ("T", 4, 0, 1), ("T", 3, 0, 2), ("T", 1, 1, 3), ("norm", 2),
    ("T", 0, 0, 4), ("T", 6, 1, 1), ("T", 0, 1, 3), ("T", 5, 0, 3), ("T", 1, 0, 4), ("T", 3, 0, 3),
    ("sc", 3), ("T", 4, 0, 2), ("T", 5, 1, 1), ("sc", 4), ("T", 2, 0, 3), ("T", 1, 1, 4), ("T", 0, 1, 4),
    ("T", 5, 1, 2), ("T", 4, 0, 3), ("T", 4, 1, 3), ("T", 0, 0, 5), ("T", 2, 1, 3), ("T", 1, 0, 5),
    ("sc", 5), ("T", 6, 0, 2), ("T", 3, 1, 3), ("T", 2, 0, 4), ("T", 0, 1, 5), ("mix", 0), ("T", 1, 1, 5),
    ("T", 4, 0, 4), ("mix", 1), ("pool", 0), ("pool", 1), ("share", 1), ("T", 3, 0, 4), ("pool", 2),
    ("share", 0), ("mid", 0), ("T", 2, 0, 5), ("pool", 3), ("share", 3), ("T", 2, 1, 4), ("share", 2),
    ("T", 6, 0, 3), ("mid", 2), ("T", 4, 1, 4), ("T", 6, 1, 2), ("mid", 1), ("T", 5, 1, 3), ("mid", 3),
    ("up", 1, 0), ("T", 4, 0, 5), ("T", 3, 1, 4), ("T", 2, 1, 5), ("up", 1, 1), ("T", 4, 1, 5),
    ("dn", 4, 3), ("T", 6, 0, 4), ("T", 6, 1, 3), ("dn", 4, 2), ("T", 5, 1, 4), ("dn", 4, 1), ("dn", 4, 0),
    ("T", 5, 0, 4), ("T", 3, 1, 5), ("up", 2, 1), ("T", 3, 0, 5), ("T", 6, 1, 4), ("up", 2, 0),
    ("T", 5, 1, 5), ("T", 5, 0, 5), ("dn", 5, 2), ("dn", 5, 0), ("dn", 5, 1), ("dn", 5, 3), ("T", 6, 0, 5),
    ("T", 6, 1, 5), ("last", 0), ("last", 1), ("own", 0), ("total", 0), ("total", 1), ("own", 1),
    ("total", 2), ("total", 3), ("final", 0), ("final", 1), ("final", 2), ("final", 3),
)
ORDERS = (
    ("xyz", "xzy"),
    ("xyz", "xyz"),
    ("xyz", "xzy"),
    ("xyz", "xzy"),
    ("xyz", "xzy"),
    ("xzy", "xzy"),
    ("xyz", "zxy"),
)


def dot(a, b):
    return jnp.dot(a, b, preferred_element_type=F32)


def dot_t(a, b):
    return lax.dot_general(a, b, (((1,), (1,)), ((), ())), preferred_element_type=F32)


def spot():
    return dict(
        z=lax.axis_index("rep") * 2 + lax.axis_index("fs_0"),
        y=lax.axis_index("fs_1"),
        x=lax.axis_index("fs_2"),
        t=lax.axis_index("tp"),
    )


def to(axis, at):
    if axis == "x":
        return {"fs_2": at}
    if axis == "y":
        return {"fs_1": at}
    if axis == "z":
        return {"rep": at // 2, "fs_0": at % 2}
    return {"tp": at}


def send(src, dst, send_sem, recv_sem, axis, at):
    return pltpu.make_async_remote_copy(
        src_ref=src,
        dst_ref=dst,
        send_sem=send_sem,
        recv_sem=recv_sem,
        device_id=to(axis, at),
        device_id_type=MESH,
    )


class Gather:
    def __init__(self, bufs, send_sem, recv_sem, me):
        self.bufs, self.send_sem, self.recv_sem, self.me = bufs, send_sem, recv_sem, me
        self.on_way, self.unused = {}, list(range(POOL))
        self.steps = {
            (b, p): self.plan(b, p, order) for b in range(NB) for p, order in enumerate(ORDERS[b])
        }

    def region(self, b, c, at, half=None, colours=1):
        buf, row, rows, lane, width, row_step, step = BATCHES[b]
        row, lane = row + row_step * c, lane + step * c
        rows, width = rows + row_step * (colours - 1), width + step * (colours - 1)
        if half is not None:
            lane, width = lane + width // 2 * half, width // 2
        return self.bufs[buf].at[at["z"], at["y"], at["x"], pl.ds(row, rows), pl.ds(lane, width)]

    def plan(self, b, p, order):
        me = self.me
        owns = [dict(z=me["z"] % 2, y=me["y"], x=me["x"])] * 2
        steps = []
        for axis in order:
            if axis == "z":
                copies = []
                for k, d in enumerate((1, 3)):
                    ref = self.region(b, 2 * p + k, owns[k])
                    copies.append((ref, "z", lax.rem(me["z"] + d, 4)))
                steps.append((copies, self.region(b, 2 * p, owns[0], colours=2)))
            else:
                first, second = [], []
                for k in range(2):
                    along = axis if k == 0 else {"x": "y", "y": "x"}[axis]
                    up, down = lax.rem(me[along] + 1, 4), lax.rem(me[along] + 3, 4)

                    def part(i, half=None):
                        return self.region(b, 2 * p + k, {**owns[k], along: i}, half)

                    first += [(part(me[along]), along, up), (part(me[along]), along, down)]
                    second += [(part(down, 0), along, up), (part(up, 1), along, down)]
                two = self.region(b, 2 * p, {**owns[0], axis: pl.ds(0, 2)}, colours=2)
                steps.append((first, two))
                steps.append((second, self.region(b, 2 * p, owns[0], colours=2)))
            owns = [{**own, axis if k == 0 else {"x": "y", "y": "x", "z": "z"}[axis]: ALL} for k, own in enumerate(owns)]
        return steps

    def start(self, key, src, dst, recv_sem, axis, at):
        pool = self.unused.pop(0)
        copy = send(src, dst, self.send_sem.at[pool], recv_sem, axis, at)
        copy.start()
        self.on_way.setdefault(key, []).append((pool, copy))

    def arrived(self, key, ref, recv_sem):
        send(ref, ref, self.send_sem.at[0], recv_sem, "t", 1 - self.me["t"]).wait_recv()
        for pool, copy in self.on_way.pop(key):
            copy.wait_send()
            self.unused.append(pool)

    def tick(self, b, p, s):
        if s > 0:
            ref = self.steps[b, p][s - 1][1]
            self.arrived((b, p, s - 1), ref, self.recv_sem.at[b, p, s - 1])
        if s < 5:
            for ref, axis, at in self.steps[b, p][s][0]:
                self.start((b, p, s), ref, ref, self.recv_sem.at[b, p, s], axis, at)


def greet(me, wait):
    barrier = pltpu.get_barrier_semaphore()
    peers = [("x", 1), ("x", 2), ("x", 3), ("y", 1), ("y", 2), ("y", 3), ("z", 1), ("z", 3)]
    if wait:
        pl.semaphore_wait(barrier, len(peers) + 1)
        return
    for axis, d in peers:
        pl.semaphore_signal(
            barrier, inc=1, device_id=to(axis, lax.rem(me[axis] + d, 4)), device_id_type=MESH
        )
    pl.semaphore_signal(barrier, inc=1, device_id=to("t", 1 - me["t"]), device_id_type=MESH)


def kernel(
    tokens,
    gains_in,
    mix_in,
    group_in,
    up_in,
    down_in,
    mix_s_in,
    group_s_in,
    up_s_in,
    down_s_in,
    out,
    gains,
    mix_w,
    group_w,
    up_w,
    down_w,
    mix_s,
    group_s,
    up_s,
    down_s,
    w0,
    w1,
    w2,
    w3,
    w4,
    x_buf,
    normed,
    mixed,
    branch,
    hidden,
    acc,
    part_out,
    part_in,
    squares,
    band,
    tile,
    sc_in,
    sc_sum,
    scale,
    inverses,
    g_send,
    g_recv,
    load_sem,
    p_recv,
    s_recv,
):
    me = spot()
    greet(me, False)
    t, other = me["t"], 1 - me["t"]
    here = (me["z"] % 2, me["y"], me["x"])
    bufs = (w0, w1, w2, w3, w4)
    gather = Gather(bufs, g_send, g_recv, me)

    def rows_of(i, size=BLOCK):
        return pl.ds(i * size, size)

    def scale_tile():
        place = me["z"] % 2 * 16 + me["y"] * 4 + me["x"]
        lane = lax.broadcasted_iota(jnp.int32, (1, 128), 1)
        base = 0
        for ref in (mix_s, group_s, up_s, down_s):
            n = ref.shape[1] // 2
            q = lax.broadcasted_iota(jnp.int32, (n, 2 * n), 0)
            r = lax.broadcasted_iota(jnp.int32, (n, 2 * n), 1)
            value = jnp.zeros((n, 128), F32)
            for j in range(2):
                for h in range(2):
                    own = jnp.where(r == 2 * q + h, ref[j : j + 1], 0.0)
                    column = jnp.sum(own, axis=1, keepdims=True)
                    value = value + jnp.where(lane == h * 64 + 2 * place + j, column, 0.0)
            tile[base : base + n] = value
            base += n

    def load(k, src, dst):
        copy = pltpu.make_async_copy(src, dst, load_sem.at[k])
        copy.start()
        return copy

    pairs = (
        (mix_in, mix_w),
        (group_in, group_w),
        (mix_s_in, mix_s),
        (group_s_in, group_s),
        (up_s_in, up_s),
        (down_s_in, down_s),
        (up_in, up_w),
        (down_in, down_w),
        (gains_in, gains),
    )
    early = [load(k, src, dst) for k, (src, dst) in enumerate(pairs)]
    own_tokens = load(len(pairs), tokens, x_buf.at[t])
    for copy in early[:6]:
        copy.wait()
    w0[here[0], here[1], here[2], 0:64] = mix_w[...].astype(BF16)
    w0[here[0], here[1], here[2], 64:80, 0:GW] = group_w[0].astype(BF16)
    w0[here[0], here[1], here[2], 64:80, GW:] = group_w[1].astype(BF16)
    scale_tile()
    for copy in early[6:]:
        copy.wait()
    up_all, down_all = up_w[...].astype(BF16), down_w[...].astype(BF16)
    for ref, lane in ((w1, 0), (w2, 1024)):
        ref[here[0], here[1], here[2]] = up_all[:, lane : lane + 1024]
    for ref, lane in ((w3, 0), (w4, 1024)):
        ref[here[0], here[1], here[2]] = down_all[:, lane : lane + 1024]
    with jax.named_scope("greet"):
        greet(me, True)

    def share(kind, i, src, dst):
        gather.start((kind, i), src, dst, p_recv.at[kind, i], "t", other)

    def arrived(kind, i, ref):
        gather.arrived((kind, i), ref, p_recv.at[kind, i])

    for p in range(2):
        gather.tick(0, p, 0)
    share(0, 0, tokens, x_buf.at[t])

    def scales(step):
        if step == 0:
            for d in (1, 2, 3):
                at = lax.rem(me["x"] + d, 4)
                gather.start("sx", tile, sc_in.at[d - 1], s_recv.at[0], "x", at)
        if step == 1:
            gather.arrived("sx", sc_in.at[0:3], s_recv.at[0])
            sc_sum[0] = tile[...] + sc_in[0] + sc_in[1] + sc_in[2]
        if step == 2:
            for d in (1, 2, 3):
                at = lax.rem(me["y"] + d, 4)
                gather.start("sy", sc_sum.at[0], sc_in.at[d + 2], s_recv.at[1], "y", at)
        if step == 3:
            gather.arrived("sy", sc_in.at[3:6], s_recv.at[1])
            sc_sum[1] = sc_sum[0] + sc_in[3] + sc_in[4] + sc_in[5]
        if step == 4:
            at = me["z"] + 1 - 2 * (me["z"] % 2)
            gather.start("sz", sc_sum.at[1], sc_in.at[6], s_recv.at[2], "z", at)
        if step == 5:
            gather.arrived("sz", sc_in.at[6], s_recv.at[2])
            whole = sc_sum[1] + sc_in[6]
            for q in range(40):
                scale[q // 8 : q // 8 + 1, 128 * (q % 8) : 128 * (q % 8) + 128] = whole[q : q + 1]

    def bands():
        i = lax.broadcasted_iota(jnp.int32, (BLOCK, 2 * BLOCK), 0)
        j = lax.broadcasted_iota(jnp.int32, (BLOCK, 2 * BLOCK), 1) - BLOCK
        for g, window in enumerate((2 + 6 * t, 4 + 12 * t)):
            band[g] = jnp.where((j <= i) & (j > i - window), 1.0, 0.0).astype(BF16)

    def mean_inverse(total):
        return lax.rsqrt(total * (1.0 / (2 * HALF)) + EPS)

    def row_sum(v):
        return jnp.sum(v, axis=1, keepdims=True)

    SUB, UNROLL = 16, 4

    def first_norm(i):
        if i == 0:
            own_tokens.wait()
            arrived(0, 0, x_buf.at[other])
        g0, g1 = gains[0:1, 0:HALF], gains[0:1, HALF:]

        def body(k, _):
            rows = pl.ds(pl.multiple_of(i * BLOCK + k * SUB, SUB), SUB)
            a, b = x_buf[0, rows].astype(F32), x_buf[1, rows].astype(F32)
            inverse = mean_inverse(row_sum(a * a + b * b))
            normed[rows, 0:HALF] = (a * inverse * g0).astype(BF16)
            normed[rows, HALF:] = (b * inverse * g1).astype(BF16)
            return 0

        lax.fori_loop(0, BLOCK // SUB, body, 0, unroll=UNROLL)

    def mix(p):
        cols = slice(GW * p, GW * p + GW)
        weight = w0[:, :, :, 0:64, cols].reshape(2 * HALF, GW)
        mixed[:, cols] = (dot(normed[...], weight) * scale[0:1, cols]).astype(BF16)

    def pool(i):
        rows = slice(i * BLOCK, i * BLOCK + BLOCK)
        for g in range(2):
            cols = slice(GW * g, GW * g + GW)
            window = (2 + 6 * t, 4 + 12 * t)[g]
            own = mixed[rows, cols]
            if i == 0:
                sums = dot(band[g, :, BLOCK:], own)
                position = lax.broadcasted_iota(jnp.int32, (BLOCK, 1), 0)
                sums = sums / jnp.minimum(position + 1, window).astype(F32)
            else:
                sums = dot(band[g], mixed[rows.start - BLOCK : rows.stop, cols])
                sums = sums * (1.0 / jnp.full((BLOCK, 1), window, jnp.int32).astype(F32))
            pooled = (sums - own.astype(F32)).astype(BF16)
            weight = w0[:, :, :, 64:80, cols].reshape(GW, GW)
            branch[t, rows, cols] = (dot(pooled, weight) * scale[1:2, cols]).astype(BF16)

    def branch_share(i):
        share(1, i, branch.at[t, rows_of(i)], branch.at[t, rows_of(i)])

    def middle(i):
        arrived(1, i, branch.at[other, rows_of(i)])
        post = [gains[1:2, 0:HALF], gains[1:2, HALF:]]
        pre = [gains[2:3, 0:HALF], gains[2:3, HALF:]]

        def body(k, _):
            rows = pl.ds(pl.multiple_of(i * BLOCK + k * SUB, SUB), SUB)
            parts = [branch[h, rows].astype(F32) for h in range(2)]
            inverse = mean_inverse(row_sum(parts[0] * parts[0] + parts[1] * parts[1]))
            mids = []
            for h in range(2):
                add = (parts[h] * inverse * post[h]).astype(BF16).astype(F32)
                mid = (x_buf[h, rows].astype(F32) + add).astype(BF16)
                x_buf[h, rows] = mid
                mids.append(mid.astype(F32))
            inverse = mean_inverse(row_sum(mids[0] * mids[0] + mids[1] * mids[1]))
            for h in range(2):
                normed[rows, h * HALF : h * HALF + HALF] = (mids[h] * inverse * pre[h]).astype(BF16)
            return 0

        lax.fori_loop(0, BLOCK // SUB, body, 0, unroll=UNROLL)

    def up(buf, p):
        cols = slice(512 * p, 512 * p + 512)
        place = slice((buf - 1) * 1024 + 512 * p, (buf - 1) * 1024 + 512 * p + 512)
        weight = bufs[buf][:, :, :, :, cols].reshape(2 * HALF, 512)
        act = jnp.maximum(dot(normed[...], weight) * scale[buf + 1 : buf + 2, cols], 0.0)
        hidden[:, place] = (act * act).astype(BF16)

    def down(b, n, part=None):
        buf, lane, width = ((3, 0, 1024), (4, 0, KCUT), (4, KCUT, 1024 - KCUT))[b - 4]
        half, k = (other, n) if n < 2 else (t, n - 2)
        first = (buf - 3) * 1024 + lane
        weight = bufs[buf][half, 2 * k : 2 * k + 2, :, :, lane : lane + width]
        weight = weight.reshape(512, width)
        cols = slice(512 * k, 512 * k + 512)

        def body(i, _):
            rows = pl.ds(pl.multiple_of(i * MROWS, MROWS), MROWS)
            value = dot_t(hidden[rows, first : first + width], weight)
            if buf > 3:
                value = value + acc[half, rows, cols]
            if b < NB - 1:
                acc[half, rows, cols] = value
            elif n < 2:
                part_out[rows, cols] = value.astype(BF16)
            else:
                mixed[rows, cols] = value.astype(BF16)
            return 0

        if part is not None:
            body(part, 0)
        else:
            lax.fori_loop(0, LENGTH // MROWS, body, 0)

    def last(part):
        for n in range(2):
            down(NB - 1, n, part)
        share(2, part, part_out.at[rows_of(part, 512)], part_in.at[rows_of(part, 512)])

    def last_own(part):
        for n in range(2, 4):
            down(NB - 1, n, part)

    def total(i):
        if i % 2 == 0:
            arrived(2, i // 2, part_in.at[rows_of(i // 2, 512)])

        def body(k, _):
            rows = pl.ds(pl.multiple_of(i * BLOCK + k * SUB, SUB), SUB)
            both = mixed[rows].astype(F32) + part_in[rows].astype(F32)
            value = (both * scale[4:5]).astype(BF16)
            mixed[rows] = value
            value = value.astype(F32)
            square = value * value
            lanes = square[:, 0:128]
            for q in range(1, 8):
                lanes = lanes + square[:, 128 * q : 128 * q + 128]
            squares[t, rows] = lanes
            return 0

        lax.fori_loop(0, BLOCK // SUB, body, 0, unroll=UNROLL)
        share(3, i, squares.at[t, rows_of(i)], squares.at[t, rows_of(i)])

    def final(i):
        arrived(3, i, squares.at[other, rows_of(i)])
        gain = gains[3:4, pl.ds(pl.multiple_of(t * HALF, HALF), HALF)]
        squared = squares[0, rows_of(i)] + squares[1, rows_of(i)]
        inverses[...] = jnp.broadcast_to(mean_inverse(row_sum(squared)), (BLOCK, 128))

        def body(k, _):
            at = pl.ds(pl.multiple_of(k * SUB, SUB), SUB)
            rows = pl.ds(pl.multiple_of(i * BLOCK + k * SUB, SUB), SUB)
            inverse = jnp.concatenate([inverses[at]] * (HALF // 128), axis=1)
            add = (mixed[rows].astype(F32) * inverse * gain).astype(BF16).astype(F32)
            out[rows] = (x_buf[t, rows].astype(F32) + add).astype(BF16)
            return 0

        lax.fori_loop(0, BLOCK // SUB, body, 0, unroll=UNROLL)

    def run(name, step, *args):
        with jax.named_scope(name):
            step(*args)

    steps = dict(
        sc=scales, bands=bands, norm=first_norm, mix=mix, pool=pool, mid=middle, up=up, dn=down
    )
    steps.update(T=gather.tick, share=branch_share, total=total, final=final)
    steps.update(last=last, own=last_own)
    run("sc", scales, 0)
    for name, *args in PLAN:
        run("#".join(map(str, (name, *args))), steps[name], *args)


def on_device(
    tokens,
    norm_gains,
    mix_weight,
    mix_scale,
    group_weight,
    group_scale,
    up_weight,
    up_scale,
    down_weight,
    down_scale,
):
    arrays = (tokens, norm_gains, mix_weight, group_weight, up_weight, down_weight.T)
    arrays += (mix_scale.T, group_scale.T, up_scale.T, down_scale.T)
    dma = pltpu.SemaphoreType.DMA
    return pl.pallas_call(
        kernel,
        out_shape=pltpu.VMEM((LENGTH, HALF), BF16),
        in_specs=[pl.BlockSpec(memory_space=pl.ANY)] + [pl.BlockSpec(memory_space=pl.ANY)] * 9,
        out_specs=pl.BlockSpec(memory_space=pltpu.VMEM),
        scratch_shapes=[pltpu.VMEM(a.shape, F32) for a in arrays[1:]]
        + [pltpu.VMEM((2, 4, 4, r, 1024), BF16) for r in ROWS]
        + [
            pltpu.VMEM((2, LENGTH, HALF), BF16),
            pltpu.VMEM((LENGTH, 2 * HALF), BF16),
            pltpu.VMEM((LENGTH, HALF), BF16),
            pltpu.VMEM((2, LENGTH, HALF), BF16),
            pltpu.VMEM((LENGTH, 2048), BF16),
            pltpu.VMEM((2, LENGTH, HALF), F32),
            pltpu.VMEM((LENGTH, HALF), BF16),
            pltpu.VMEM((LENGTH, HALF), BF16),
            pltpu.VMEM((2, LENGTH, 128), F32),
            pltpu.VMEM((2, BLOCK, 2 * BLOCK), BF16),
            pltpu.VMEM((40, 128), F32),
            pltpu.VMEM((7, 40, 128), F32),
            pltpu.VMEM((2, 40, 128), F32),
            pltpu.VMEM((5, 1024), F32),
            pltpu.VMEM((BLOCK, 128), F32),
            dma((POOL,)),
            dma((NB, 2, 5)),
            dma((10,)),
            dma((4, NR)),
            dma((3,)),
        ],
        compiler_params=pltpu.CompilerParams(
            collective_id=0, has_side_effects=True, vmem_limit_bytes=60_000_000
        ),
    )(*arrays)


def solution(mesh):
    finer = Mesh(
        mesh.devices.reshape(mesh.shape["rep"], 2, 4, 4, mesh.shape["tp"]),
        ("rep", "fs_0", "fs_1", "fs_2", "tp"),
    )
    in_specs = (
        P(REP_FS, "tp"),
        P(),
        P(FS, "tp"),
        P("tp", FS),
        P("tp", FS, None),
        P("tp", FS),
        P(FS, "tp"),
        P("tp", FS),
        P("tp", FS),
        P("tp", FS),
    )
    out_specs = P(REP_FS, "tp")
    return jax.shard_map(
        on_device, mesh=finer, in_specs=in_specs, out_specs=out_specs, check_vma=False
    )
```

```python
import functools

import jax
import jax.numpy as jnp
from jax import lax
from jax.experimental import pallas as pl
from jax.experimental.pallas import tpu as pltpu
from jax.sharding import Mesh
from jax.sharding import PartitionSpec as P

FS = ("fs_0", "fs_1", "fs_2")
REP_FS = ("rep", "fs_0", "fs_1", "fs_2")
MESH = pl.DeviceIdType.MESH
ALL = slice(None)
EPS = 1e-06

LENGTH = 1024
HALF = 1024
GW = 512
ROWS = (80, 64, 64, 64, 64)
KCUT = 512
BATCHES = (
    (0, 0, 64, 0, 256, 0, 256),
    (0, 64, 16, 0, 256, 0, 256),
    (1, 0, 64, 0, 256, 0, 256),
    (2, 0, 64, 0, 256, 0, 256),
    (3, 0, 64, 0, 256, 0, 256),
    (4, 0, 16, 0, KCUT, 16, 0),
    (4, 0, 16, KCUT, 1024 - KCUT, 16, 0),
)
NB = len(BATCHES)
POOL = 16
MROWS = 512
BLOCK = 256
NR = LENGTH // BLOCK
F32, BF16 = jnp.float32, jnp.bfloat16


PLAN = (
    ("bands",), ("T", 2, 0, 0), ("T", 1, 0, 0), ("T", 1, 1, 0), ("T", 6, 0, 0), ("T", 5, 0, 0),
    ("T", 4, 0, 0), ("T", 5, 1, 0), ("T", 4, 1, 0), ("T", 3, 1, 0), ("T", 0, 0, 1), ("sc", 1), ("sc", 2),
    ("T", 0, 1, 1), ("T", 2, 1, 0), ("T", 6, 1, 0), ("T", 3, 0, 0), ("T", 5, 0, 1), ("T", 1, 1, 1),
    ("T", 4, 0, 1), ("T", 6, 0, 1), ("T", 2, 0, 1), ("T", 1, 0, 1), ("T", 4, 1, 1), ("norm", 0),
    ("T", 3, 1, 1), ("T", 0, 0, 2), ("T", 5, 1, 1), ("T", 0, 1, 2), ("T", 3, 0, 1), ("norm", 1),
    ("T", 5, 0, 2), ("T", 6, 1, 1), ("norm", 3), ("T", 1, 1, 2), ("T", 1, 0, 2), ("T", 4, 1, 2), ("sc", 3),
    ("T", 5, 1, 2), ("sc", 4), ("T", 2, 1, 1), ("T", 2, 0, 2), ("T", 3, 1, 2), ("T", 0, 1, 3),
    ("T", 0, 0, 3), ("T", 1, 1, 3), ("T", 4, 0, 2), ("T", 1, 0, 3), ("T", 6, 1, 2), ("T", 0, 1, 4),
    ("T", 2, 0, 3), ("T", 4, 0, 3), ("T", 1, 1, 4), ("T", 2, 1, 2), ("T", 3, 0, 2), ("T", 1, 0, 4),
    ("T", 0, 0, 4), ("T", 2, 0, 4), ("norm", 2), ("T", 2, 1, 3), ("T", 5, 0, 3), ("T", 3, 0, 3), ("sc", 5),
    ("T", 6, 1, 3), ("T", 6, 0, 2), ("T", 4, 1, 3), ("T", 1, 1, 5), ("T", 2, 1, 4), ("T", 0, 0, 5),
    ("T", 0, 1, 5), ("mix", 0), ("T", 1, 0, 5), ("T", 3, 1, 3), ("mix", 1), ("pool", 0), ("pool", 1),
    ("pool", 2), ("T", 4, 0, 4), ("pool", 3), ("share", 3), ("share", 1), ("T", 4, 1, 4), ("T", 5, 1, 3),
    ("share", 0), ("mid", 3), ("share", 2), ("mid", 1), ("T", 2, 0, 5), ("T", 3, 0, 4), ("mid", 0),
    ("mid", 2), ("up", 1, 0), ("T", 3, 1, 4), ("T", 6, 1, 4), ("T", 4, 0, 5), ("T", 2, 1, 5),
    ("T", 6, 0, 3), ("up", 1, 1), ("T", 4, 1, 5), ("dn", 4, 0), ("dn", 4, 1), ("dn", 4, 2), ("T", 5, 1, 4),
    ("dn", 4, 3), ("T", 5, 0, 4), ("T", 3, 1, 5), ("up", 2, 1), ("T", 6, 0, 4), ("T", 3, 0, 5),
    ("up", 2, 0), ("T", 5, 1, 5), ("T", 5, 0, 5), ("dn", 5, 1), ("dn", 5, 2), ("dn", 5, 3), ("dn", 5, 0),
    ("T", 6, 0, 5), ("T", 6, 1, 5), ("last", 0), ("last", 1), ("own", 0), ("total", 0), ("total", 1),
    ("own", 1), ("total", 2), ("total", 3), ("final", 0), ("final", 1), ("final", 2), ("final", 3),
)
ORDERS = (
    ("xzy", "xyz"),
    ("xyz", "xyz"),
    ("xyz", "xyz"),
    ("xyz", "xzy"),
    ("xzy", "xzy"),
    ("xzy", "xzy"),
    ("zxy", "xyz"),
)


def dot(a, b):
    return jnp.dot(a, b, preferred_element_type=F32)


def dot_t(a, b):
    return lax.dot_general(a, b, (((1,), (1,)), ((), ())), preferred_element_type=F32)


def spot():
    return dict(
        z=lax.axis_index("rep") * 2 + lax.axis_index("fs_0"),
        y=lax.axis_index("fs_1"),
        x=lax.axis_index("fs_2"),
        t=lax.axis_index("tp"),
    )


def to(axis, at):
    if axis == "x":
        return {"fs_2": at}
    if axis == "y":
        return {"fs_1": at}
    if axis == "z":
        return {"rep": at // 2, "fs_0": at % 2}
    return {"tp": at}


def send(src, dst, send_sem, recv_sem, axis, at):
    return pltpu.make_async_remote_copy(
        src_ref=src,
        dst_ref=dst,
        send_sem=send_sem,
        recv_sem=recv_sem,
        device_id=to(axis, at),
        device_id_type=MESH,
    )


class Gather:
    def __init__(self, bufs, send_sem, recv_sem, me):
        self.bufs, self.send_sem, self.recv_sem, self.me = bufs, send_sem, recv_sem, me
        self.on_way, self.unused = {}, list(range(POOL))
        self.steps = {
            (b, p): self.plan(b, p, order) for b in range(NB) for p, order in enumerate(ORDERS[b])
        }

    def region(self, b, c, at, half=None, colours=1):
        buf, row, rows, lane, width, row_step, step = BATCHES[b]
        row, lane = row + row_step * c, lane + step * c
        rows, width = rows + row_step * (colours - 1), width + step * (colours - 1)
        if half is not None:
            lane, width = lane + width // 2 * half, width // 2
        return self.bufs[buf].at[at["z"], at["y"], at["x"], pl.ds(row, rows), pl.ds(lane, width)]

    def plan(self, b, p, order):
        me = self.me
        owns = [dict(z=me["z"] % 2, y=me["y"], x=me["x"])] * 2
        steps = []
        for axis in order:
            if axis == "z":
                copies = []
                for k, d in enumerate((1, 3)):
                    ref = self.region(b, 2 * p + k, owns[k])
                    copies.append((ref, "z", lax.rem(me["z"] + d, 4)))
                steps.append((copies, self.region(b, 2 * p, owns[0], colours=2)))
            else:
                first, second = [], []
                for k in range(2):
                    along = axis if k == 0 else {"x": "y", "y": "x"}[axis]
                    up, down = lax.rem(me[along] + 1, 4), lax.rem(me[along] + 3, 4)

                    def part(i, half=None):
                        return self.region(b, 2 * p + k, {**owns[k], along: i}, half)

                    first += [(part(me[along]), along, up), (part(me[along]), along, down)]
                    second += [(part(down, 0), along, up), (part(up, 1), along, down)]
                two = self.region(b, 2 * p, {**owns[0], axis: pl.ds(0, 2)}, colours=2)
                steps.append((first, two))
                steps.append((second, self.region(b, 2 * p, owns[0], colours=2)))
            owns = [{**own, axis if k == 0 else {"x": "y", "y": "x", "z": "z"}[axis]: ALL} for k, own in enumerate(owns)]
        return steps

    def start(self, key, src, dst, recv_sem, axis, at):
        if key not in self.on_way:
            self.on_way[key] = self.unused.pop(0)
        send(src, dst, self.send_sem.at[self.on_way[key]], recv_sem, axis, at).start()

    def arrived(self, key, ref, recv_sem):
        pool = self.on_way.pop(key)
        copies = send(ref, ref, self.send_sem.at[pool], recv_sem, "t", 1 - self.me["t"])
        copies.wait_recv()
        copies.wait_send()
        self.unused.append(pool)

    def tick(self, b, p, s):
        if s > 0:
            ref = self.steps[b, p][s - 1][1]
            self.arrived((b, p, s - 1), ref, self.recv_sem.at[b, p, s - 1])
        if s < 5:
            for ref, axis, at in self.steps[b, p][s][0]:
                self.start((b, p, s), ref, ref, self.recv_sem.at[b, p, s], axis, at)


def greet(me, wait):
    barrier = pltpu.get_barrier_semaphore()
    peers = [("x", 1), ("x", 2), ("x", 3), ("y", 1), ("y", 2), ("y", 3), ("z", 1), ("z", 3)]
    if wait:
        pl.semaphore_wait(barrier, len(peers) + 1)
        return
    for axis, d in peers:
        pl.semaphore_signal(
            barrier, inc=1, device_id=to(axis, lax.rem(me[axis] + d, 4)), device_id_type=MESH
        )
    pl.semaphore_signal(barrier, inc=1, device_id=to("t", 1 - me["t"]), device_id_type=MESH)


def kernel(
    tokens,
    gains_in,
    mix_in,
    group_in,
    up_in,
    down_in,
    mix_s_in,
    group_s_in,
    up_s_in,
    down_s_in,
    out,
    gains,
    mix_w,
    group_w,
    up_w,
    down_w,
    mix_s,
    group_s,
    up_s,
    down_s,
    w0,
    w1,
    w2,
    w3,
    w4,
    x_buf,
    normed,
    mixed,
    branch,
    hidden,
    acc,
    part_out,
    part_in,
    squares,
    band,
    tile,
    sc_in,
    sc_sum,
    scale,
    inverses,
    g_send,
    g_recv,
    load_sem,
    p_recv,
    s_recv,
):
    me = spot()
    greet(me, False)
    t, other = me["t"], 1 - me["t"]
    here = (me["z"] % 2, me["y"], me["x"])
    bufs = (w0, w1, w2, w3, w4)
    gather = Gather(bufs, g_send, g_recv, me)

    def rows_of(i, size=BLOCK):
        return pl.ds(i * size, size)

    def scale_tile():
        place = me["z"] % 2 * 16 + me["y"] * 4 + me["x"]
        lane = lax.broadcasted_iota(jnp.int32, (1, 128), 1)
        base = 0
        for ref in (mix_s, group_s, up_s, down_s):
            n = ref.shape[1] // 2
            q = lax.broadcasted_iota(jnp.int32, (n, 2 * n), 0)
            r = lax.broadcasted_iota(jnp.int32, (n, 2 * n), 1)
            value = jnp.zeros((n, 128), F32)
            for j in range(2):
                for h in range(2):
                    own = jnp.where(r == 2 * q + h, ref[j : j + 1], 0.0)
                    column = jnp.sum(own, axis=1, keepdims=True)
                    value = value + jnp.where(lane == h * 64 + 2 * place + j, column, 0.0)
            tile[base : base + n] = value
            base += n

    def load(k, src, dst):
        copy = pltpu.make_async_copy(src, dst, load_sem.at[k])
        copy.start()
        return copy

    pairs = (
        (mix_in, mix_w),
        (group_in, group_w),
        (up_in, up_w),
        (down_in, down_w),
        (gains_in, gains),
        (mix_s_in, mix_s),
        (group_s_in, group_s),
        (up_s_in, up_s),
        (down_s_in, down_s),
    )
    early = [load(k, src, dst) for k, (src, dst) in enumerate(pairs)]
    own_tokens = load(len(pairs), tokens, x_buf.at[t])
    early[0].wait()
    w0[here[0], here[1], here[2], 0:64] = mix_w[...].astype(BF16)
    with jax.named_scope("greet"):
        greet(me, True)

    def share(kind, i, src, dst):
        gather.start((kind, i), src, dst, p_recv.at[kind, i], "t", other)

    def arrived(kind, i, ref):
        gather.arrived((kind, i), ref, p_recv.at[kind, i])

    for p in range(2):
        gather.tick(0, p, 0)
    share(0, 0, tokens, x_buf.at[t])

    for copy in early[5:]:
        copy.wait()
    scale_tile()
    early[1].wait()
    w0[here[0], here[1], here[2], 64:80, 0:GW] = group_w[0].astype(BF16)
    w0[here[0], here[1], here[2], 64:80, GW:] = group_w[1].astype(BF16)
    early[2].wait()
    up_all = up_w[...].astype(BF16)
    for ref, lane in ((w1, 0), (w2, 1024)):
        ref[here[0], here[1], here[2]] = up_all[:, lane : lane + 1024]
    early[3].wait()
    down_all = down_w[...].astype(BF16)
    for ref, lane in ((w3, 0), (w4, 1024)):
        ref[here[0], here[1], here[2]] = down_all[:, lane : lane + 1024]
    early[4].wait()

    def scales(step):
        if step == 0:
            for d in (1, 2, 3):
                at = lax.rem(me["x"] + d, 4)
                gather.start("sx", tile, sc_in.at[d - 1], s_recv.at[0], "x", at)
        if step == 1:
            gather.arrived("sx", sc_in.at[0:3], s_recv.at[0])
            sc_sum[0] = tile[...] + sc_in[0] + sc_in[1] + sc_in[2]
        if step == 2:
            for d in (1, 2, 3):
                at = lax.rem(me["y"] + d, 4)
                gather.start("sy", sc_sum.at[0], sc_in.at[d + 2], s_recv.at[1], "y", at)
        if step == 3:
            gather.arrived("sy", sc_in.at[3:6], s_recv.at[1])
            sc_sum[1] = sc_sum[0] + sc_in[3] + sc_in[4] + sc_in[5]
        if step == 4:
            at = me["z"] + 1 - 2 * (me["z"] % 2)
            gather.start("sz", sc_sum.at[1], sc_in.at[6], s_recv.at[2], "z", at)
        if step == 5:
            gather.arrived("sz", sc_in.at[6], s_recv.at[2])
            whole = sc_sum[1] + sc_in[6]
            for q in range(40):
                scale[q // 8 : q // 8 + 1, 128 * (q % 8) : 128 * (q % 8) + 128] = whole[q : q + 1]

    def bands():
        i = lax.broadcasted_iota(jnp.int32, (BLOCK, 2 * BLOCK), 0)
        j = lax.broadcasted_iota(jnp.int32, (BLOCK, 2 * BLOCK), 1) - BLOCK
        for g, window in enumerate((2 + 6 * t, 4 + 12 * t)):
            band[g] = jnp.where((j <= i) & (j > i - window), 1.0, 0.0).astype(BF16)

    def mean_inverse(total):
        return lax.rsqrt(total * (1.0 / (2 * HALF)) + EPS)

    def row_sum(v):
        return jnp.sum(v, axis=1, keepdims=True)

    SUB, UNROLL = 16, 4

    def first_norm(i):
        if i == 0:
            own_tokens.wait()
            arrived(0, 0, x_buf.at[other])
        g0, g1 = gains[0:1, 0:HALF], gains[0:1, HALF:]

        def body(k, _):
            rows = pl.ds(pl.multiple_of(i * BLOCK + k * SUB, SUB), SUB)
            a, b = x_buf[0, rows].astype(F32), x_buf[1, rows].astype(F32)
            inverse = mean_inverse(row_sum(a * a + b * b))
            normed[rows, 0:HALF] = (a * inverse * g0).astype(BF16)
            normed[rows, HALF:] = (b * inverse * g1).astype(BF16)
            return 0

        lax.fori_loop(0, BLOCK // SUB, body, 0, unroll=UNROLL)

    def mix(p):
        cols = slice(GW * p, GW * p + GW)
        weight = w0[:, :, :, 0:64, cols].reshape(2 * HALF, GW)
        mixed[:, cols] = (dot(normed[...], weight) * scale[0:1, cols]).astype(BF16)

    def pool(i):
        rows = slice(i * BLOCK, i * BLOCK + BLOCK)
        for g in range(2):
            cols = slice(GW * g, GW * g + GW)
            window = (2 + 6 * t, 4 + 12 * t)[g]
            own = mixed[rows, cols]
            if i == 0:
                sums = dot(band[g, :, BLOCK:], own)
                position = lax.broadcasted_iota(jnp.int32, (BLOCK, 1), 0)
                sums = sums / jnp.minimum(position + 1, window).astype(F32)
            else:
                sums = dot(band[g], mixed[rows.start - BLOCK : rows.stop, cols])
                sums = sums * (1.0 / jnp.full((BLOCK, 1), window, jnp.int32).astype(F32))
            pooled = (sums - own.astype(F32)).astype(BF16)
            weight = w0[:, :, :, 64:80, cols].reshape(GW, GW)
            branch[t, rows, cols] = (dot(pooled, weight) * scale[1:2, cols]).astype(BF16)

    def branch_share(i):
        share(1, i, branch.at[t, rows_of(i)], branch.at[t, rows_of(i)])

    def middle(i):
        arrived(1, i, branch.at[other, rows_of(i)])
        post = [gains[1:2, 0:HALF], gains[1:2, HALF:]]
        pre = [gains[2:3, 0:HALF], gains[2:3, HALF:]]

        def body(k, _):
            rows = pl.ds(pl.multiple_of(i * BLOCK + k * SUB, SUB), SUB)
            parts = [branch[h, rows].astype(F32) for h in range(2)]
            inverse = mean_inverse(row_sum(parts[0] * parts[0] + parts[1] * parts[1]))
            mids = []
            for h in range(2):
                add = (parts[h] * inverse * post[h]).astype(BF16).astype(F32)
                mid = (x_buf[h, rows].astype(F32) + add).astype(BF16)
                x_buf[h, rows] = mid
                mids.append(mid.astype(F32))
            inverse = mean_inverse(row_sum(mids[0] * mids[0] + mids[1] * mids[1]))
            for h in range(2):
                normed[rows, h * HALF : h * HALF + HALF] = (mids[h] * inverse * pre[h]).astype(BF16)
            return 0

        lax.fori_loop(0, BLOCK // SUB, body, 0, unroll=UNROLL)

    def up(buf, p):
        cols = slice(512 * p, 512 * p + 512)
        place = slice((buf - 1) * 1024 + 512 * p, (buf - 1) * 1024 + 512 * p + 512)
        weight = bufs[buf][:, :, :, :, cols].reshape(2 * HALF, 512)
        act = jnp.maximum(dot(normed[...], weight) * scale[buf + 1 : buf + 2, cols], 0.0)
        hidden[:, place] = (act * act).astype(BF16)

    def down(b, n, part=None):
        buf, lane, width = ((3, 0, 1024), (4, 0, KCUT), (4, KCUT, 1024 - KCUT))[b - 4]
        half, k = (other, n) if n < 2 else (t, n - 2)
        first = (buf - 3) * 1024 + lane
        weight = bufs[buf][half, 2 * k : 2 * k + 2, :, :, lane : lane + width]
        weight = weight.reshape(512, width)
        cols = slice(512 * k, 512 * k + 512)

        rows = ALL if part is None else pl.ds(part * MROWS, MROWS)
        value = dot_t(hidden[rows, first : first + width], weight)
        if buf > 3:
            value = value + acc[half, rows, cols]
        if b < NB - 1:
            acc[half, rows, cols] = value
        elif n < 2:
            part_out[rows, cols] = value.astype(BF16)
        else:
            mixed[rows, cols] = value.astype(BF16)

    def last(part):
        for n in range(2):
            down(NB - 1, n, part)
        share(2, part, part_out.at[rows_of(part, 512)], part_in.at[rows_of(part, 512)])

    def last_own(part):
        for n in range(2, 4):
            down(NB - 1, n, part)

    def total(i):
        if i % 2 == 0:
            arrived(2, i // 2, part_in.at[rows_of(i // 2, 512)])

        def body(k, _):
            rows = pl.ds(pl.multiple_of(i * BLOCK + k * SUB, SUB), SUB)
            both = mixed[rows].astype(F32) + part_in[rows].astype(F32)
            value = (both * scale[4:5]).astype(BF16)
            mixed[rows] = value
            value = value.astype(F32)
            square = value * value
            lanes = square[:, 0:128]
            for q in range(1, 8):
                lanes = lanes + square[:, 128 * q : 128 * q + 128]
            squares[t, rows] = lanes
            return 0

        lax.fori_loop(0, BLOCK // SUB, body, 0, unroll=UNROLL)
        share(3, i, squares.at[t, rows_of(i)], squares.at[t, rows_of(i)])

    def final(i):
        arrived(3, i, squares.at[other, rows_of(i)])
        gain = gains[3:4, pl.ds(pl.multiple_of(t * HALF, HALF), HALF)]
        squared = squares[0, rows_of(i)] + squares[1, rows_of(i)]
        inverses[...] = jnp.broadcast_to(mean_inverse(row_sum(squared)), (BLOCK, 128))

        def body(k, _):
            at = pl.ds(pl.multiple_of(k * SUB, SUB), SUB)
            rows = pl.ds(pl.multiple_of(i * BLOCK + k * SUB, SUB), SUB)
            inverse = jnp.concatenate([inverses[at]] * (HALF // 128), axis=1)
            add = (mixed[rows].astype(F32) * inverse * gain).astype(BF16).astype(F32)
            out[rows] = (x_buf[t, rows].astype(F32) + add).astype(BF16)
            return 0

        lax.fori_loop(0, BLOCK // SUB, body, 0, unroll=UNROLL)

    def run(name, step, *args):
        with jax.named_scope(name):
            step(*args)

    steps = dict(
        sc=scales, bands=bands, norm=first_norm, mix=mix, pool=pool, mid=middle, up=up, dn=down
    )
    steps.update(T=gather.tick, share=branch_share, total=total, final=final)
    steps.update(last=last, own=last_own)
    run("sc", scales, 0)
    for name, *args in PLAN:
        run("#".join(map(str, (name, *args))), steps[name], *args)


def on_device(
    tokens,
    norm_gains,
    mix_weight,
    mix_scale,
    group_weight,
    group_scale,
    up_weight,
    up_scale,
    down_weight,
    down_scale,
):
    arrays = (tokens, norm_gains, mix_weight, group_weight, up_weight, down_weight.T)
    arrays += (mix_scale.T, group_scale.T, up_scale.T, down_scale.T)
    dma = pltpu.SemaphoreType.DMA
    return pl.pallas_call(
        kernel,
        out_shape=pltpu.VMEM((LENGTH, HALF), BF16),
        in_specs=[pl.BlockSpec(memory_space=pl.ANY)] + [pl.BlockSpec(memory_space=pl.ANY)] * 9,
        out_specs=pl.BlockSpec(memory_space=pltpu.VMEM),
        scratch_shapes=[pltpu.VMEM(a.shape, F32) for a in arrays[1:]]
        + [pltpu.VMEM((2, 4, 4, r, 1024), BF16) for r in ROWS]
        + [
            pltpu.VMEM((2, LENGTH, HALF), BF16),
            pltpu.VMEM((LENGTH, 2 * HALF), BF16),
            pltpu.VMEM((LENGTH, HALF), BF16),
            pltpu.VMEM((2, LENGTH, HALF), BF16),
            pltpu.VMEM((LENGTH, 2048), BF16),
            pltpu.VMEM((2, LENGTH, HALF), F32),
            pltpu.VMEM((LENGTH, HALF), BF16),
            pltpu.VMEM((LENGTH, HALF), BF16),
            pltpu.VMEM((2, LENGTH, 128), F32),
            pltpu.VMEM((2, BLOCK, 2 * BLOCK), BF16),
            pltpu.VMEM((40, 128), F32),
            pltpu.VMEM((7, 40, 128), F32),
            pltpu.VMEM((2, 40, 128), F32),
            pltpu.VMEM((5, 1024), F32),
            pltpu.VMEM((BLOCK, 128), F32),
            dma((POOL,)),
            dma((NB, 2, 5)),
            dma((10,)),
            dma((4, NR)),
            dma((3,)),
        ],
        compiler_params=pltpu.CompilerParams(
            collective_id=0, has_side_effects=True, vmem_limit_bytes=60_000_000
        ),
    )(*arrays)


def solution(mesh):
    finer = Mesh(
        mesh.devices.reshape(mesh.shape["rep"], 2, 4, 4, mesh.shape["tp"]),
        ("rep", "fs_0", "fs_1", "fs_2", "tp"),
    )
    in_specs = (
        P(REP_FS, "tp"),
        P(),
        P(FS, "tp"),
        P("tp", FS),
        P("tp", FS, None),
        P("tp", FS),
        P(FS, "tp"),
        P("tp", FS),
        P("tp", FS),
        P("tp", FS),
    )
    out_specs = P(REP_FS, "tp")
    return jax.shard_map(
        on_device, mesh=finer, in_specs=in_specs, out_specs=out_specs, check_vma=False
    )
```

```python
import functools

import jax
import jax.numpy as jnp
from jax import lax
from jax.experimental import pallas as pl
from jax.experimental.pallas import tpu as pltpu
from jax.sharding import Mesh
from jax.sharding import PartitionSpec as P

FS = ("fs_0", "fs_1", "fs_2")
REP_FS = ("rep", "fs_0", "fs_1", "fs_2")
MESH = pl.DeviceIdType.MESH
ALL = slice(None)
EPS = 1e-06

LENGTH = 1024
HALF = 1024
GW = 512
ROWS = (80, 64, 64, 64, 64)
KCUT = 512
BATCHES = (
    (0, 0, 64, 0, 256, 0, 256),
    (0, 64, 16, 0, 256, 0, 256),
    (1, 0, 64, 0, 256, 0, 256),
    (2, 0, 64, 0, 256, 0, 256),
    (3, 0, 64, 0, 256, 0, 256),
    (4, 0, 16, 0, KCUT, 16, 0),
    (4, 0, 16, KCUT, 1024 - KCUT, 16, 0),
)
NB = len(BATCHES)
POOL = 16
MROWS = 512
BLOCK = 256
NR = LENGTH // BLOCK
F32, BF16 = jnp.float32, jnp.bfloat16


PLAN = (
    ("bands",), ("T", 2, 0, 0), ("T", 1, 0, 0), ("T", 1, 1, 0), ("T", 6, 0, 0), ("T", 5, 0, 0),
    ("T", 4, 0, 0), ("T", 5, 1, 0), ("T", 4, 1, 0), ("T", 3, 1, 0), ("T", 0, 0, 1), ("sc", 1), ("sc", 2),
    ("T", 0, 1, 1), ("T", 2, 1, 0), ("T", 6, 1, 0), ("T", 3, 0, 0), ("T", 5, 0, 1), ("T", 1, 1, 1),
    ("T", 4, 0, 1), ("T", 6, 0, 1), ("T", 2, 0, 1), ("T", 1, 0, 1), ("T", 4, 1, 1), ("norm", 0),
    ("T", 3, 1, 1), ("T", 0, 0, 2), ("T", 5, 1, 1), ("T", 0, 1, 2), ("T", 3, 0, 1), ("norm", 1),
    ("T", 5, 0, 2), ("T", 6, 1, 1), ("norm", 3), ("T", 1, 1, 2), ("T", 1, 0, 2), ("T", 4, 1, 2), ("sc", 3),
    ("T", 5, 1, 2), ("sc", 4), ("T", 2, 1, 1), ("T", 2, 0, 2), ("T", 3, 1, 2), ("T", 0, 1, 3),
    ("T", 0, 0, 3), ("T", 1, 1, 3), ("T", 4, 0, 2), ("T", 1, 0, 3), ("T", 6, 1, 2), ("T", 0, 1, 4),
    ("T", 2, 0, 3), ("T", 4, 0, 3), ("T", 1, 1, 4), ("T", 2, 1, 2), ("T", 3, 0, 2), ("T", 1, 0, 4),
    ("T", 0, 0, 4), ("T", 2, 0, 4), ("norm", 2), ("T", 2, 1, 3), ("T", 5, 0, 3), ("T", 3, 0, 3), ("sc", 5),
    ("T", 6, 1, 3), ("T", 6, 0, 2), ("T", 4, 1, 3), ("T", 1, 1, 5), ("T", 2, 1, 4), ("T", 0, 0, 5),
    ("T", 0, 1, 5), ("mix", 0), ("T", 1, 0, 5), ("T", 3, 1, 3), ("mix", 1), ("pool", 0), ("pool", 1),
    ("pool", 2), ("T", 4, 0, 4), ("pool", 3), ("share", 3), ("share", 1), ("T", 4, 1, 4), ("T", 5, 1, 3),
    ("share", 0), ("mid", 3), ("share", 2), ("mid", 1), ("T", 2, 0, 5), ("T", 3, 0, 4), ("mid", 0),
    ("mid", 2), ("up", 1, 0), ("T", 3, 1, 4), ("T", 6, 1, 4), ("T", 4, 0, 5), ("T", 2, 1, 5),
    ("T", 6, 0, 3), ("up", 1, 1), ("T", 4, 1, 5), ("dn", 4, 0), ("dn", 4, 1), ("dn", 4, 2), ("T", 5, 1, 4),
    ("dn", 4, 3), ("T", 5, 0, 4), ("T", 3, 1, 5), ("up", 2, 1), ("T", 6, 0, 4), ("T", 3, 0, 5),
    ("up", 2, 0), ("T", 5, 1, 5), ("T", 5, 0, 5), ("dn", 5, 1), ("dn", 5, 2), ("dn", 5, 3), ("dn", 5, 0),
    ("T", 6, 0, 5), ("T", 6, 1, 5), ("last", 0), ("last", 1), ("own", 0), ("total", 0), ("total", 1),
    ("own", 1), ("total", 2), ("total", 3), ("final", 0), ("final", 1), ("final", 2), ("final", 3),
)
ORDERS = (
    ("xzy", "xyz"),
    ("xyz", "xyz"),
    ("xyz", "xyz"),
    ("xyz", "xzy"),
    ("xzy", "xzy"),
    ("xzy", "xzy"),
    ("zxy", "xyz"),
)


def dot(a, b):
    return jnp.dot(a, b, preferred_element_type=F32)


def dot_t(a, b):
    return lax.dot_general(a, b, (((1,), (1,)), ((), ())), preferred_element_type=F32)


def spot():
    return dict(
        z=lax.axis_index("rep") * 2 + lax.axis_index("fs_0"),
        y=lax.axis_index("fs_1"),
        x=lax.axis_index("fs_2"),
        t=lax.axis_index("tp"),
    )


def to(axis, at):
    if axis == "x":
        return {"fs_2": at}
    if axis == "y":
        return {"fs_1": at}
    if axis == "z":
        return {"rep": at // 2, "fs_0": at % 2}
    return {"tp": at}


def send(src, dst, send_sem, recv_sem, axis, at):
    return pltpu.make_async_remote_copy(
        src_ref=src,
        dst_ref=dst,
        send_sem=send_sem,
        recv_sem=recv_sem,
        device_id=to(axis, at),
        device_id_type=MESH,
    )


class Gather:
    def __init__(self, bufs, send_sem, recv_sem, me):
        self.bufs, self.send_sem, self.recv_sem, self.me = bufs, send_sem, recv_sem, me
        self.on_way, self.unused = {}, list(range(POOL))
        self.steps = {
            (b, p): self.plan(b, p, order) for b in range(NB) for p, order in enumerate(ORDERS[b])
        }

    def region(self, b, c, at, half=None, colours=1):
        buf, row, rows, lane, width, row_step, step = BATCHES[b]
        row, lane = row + row_step * c, lane + step * c
        rows, width = rows + row_step * (colours - 1), width + step * (colours - 1)
        if half is not None:
            lane, width = lane + width // 2 * half, width // 2
        return self.bufs[buf].at[at["z"], at["y"], at["x"], pl.ds(row, rows), pl.ds(lane, width)]

    def plan(self, b, p, order):
        me = self.me
        owns = [dict(z=me["z"] % 2, y=me["y"], x=me["x"])] * 2
        steps = []
        for axis in order:
            if axis == "z":
                copies = []
                for k, d in enumerate((1, 3)):
                    ref = self.region(b, 2 * p + k, owns[k])
                    copies.append((ref, "z", lax.rem(me["z"] + d, 4)))
                steps.append((copies, self.region(b, 2 * p, owns[0], colours=2)))
            else:
                first, second = [], []
                for k in range(2):
                    along = axis if k == 0 else {"x": "y", "y": "x"}[axis]
                    up, down = lax.rem(me[along] + 1, 4), lax.rem(me[along] + 3, 4)

                    def part(i, half=None):
                        return self.region(b, 2 * p + k, {**owns[k], along: i}, half)

                    first += [(part(me[along]), along, up), (part(me[along]), along, down)]
                    second += [(part(down, 0), along, up), (part(up, 1), along, down)]
                two = self.region(b, 2 * p, {**owns[0], axis: pl.ds(0, 2)}, colours=2)
                steps.append((first, two))
                steps.append((second, self.region(b, 2 * p, owns[0], colours=2)))
            owns = [{**own, axis if k == 0 else {"x": "y", "y": "x", "z": "z"}[axis]: ALL} for k, own in enumerate(owns)]
        return steps

    def start(self, key, src, dst, recv_sem, axis, at):
        if key not in self.on_way:
            self.on_way[key] = self.unused.pop(0)
        send(src, dst, self.send_sem.at[self.on_way[key]], recv_sem, axis, at).start()

    def arrived(self, key, ref, recv_sem):
        pool = self.on_way.pop(key)
        copies = send(ref, ref, self.send_sem.at[pool], recv_sem, "t", 1 - self.me["t"])
        copies.wait_recv()
        copies.wait_send()
        self.unused.append(pool)

    def tick(self, b, p, s):
        if s > 0:
            ref = self.steps[b, p][s - 1][1]
            self.arrived((b, p, s - 1), ref, self.recv_sem.at[b, p, s - 1])
        if s < 5:
            for ref, axis, at in self.steps[b, p][s][0]:
                self.start((b, p, s), ref, ref, self.recv_sem.at[b, p, s], axis, at)


def greet(me, wait):
    barrier = pltpu.get_barrier_semaphore()
    peers = [("x", 1), ("x", 2), ("x", 3), ("y", 1), ("y", 2), ("y", 3), ("z", 1), ("z", 3)]
    if wait:
        pl.semaphore_wait(barrier, len(peers) + 1)
        return
    for axis, d in peers:
        pl.semaphore_signal(
            barrier, inc=1, device_id=to(axis, lax.rem(me[axis] + d, 4)), device_id_type=MESH
        )
    pl.semaphore_signal(barrier, inc=1, device_id=to("t", 1 - me["t"]), device_id_type=MESH)


def kernel(
    tokens,
    gains_in,
    mix_in,
    group_in,
    up_in,
    down_in,
    mix_s_in,
    group_s_in,
    up_s_in,
    down_s_in,
    out,
    gains,
    mix_w,
    group_w,
    up_w,
    down_w,
    mix_s,
    group_s,
    up_s,
    down_s,
    w0,
    w1,
    w2,
    w3,
    w4,
    x_buf,
    normed,
    mixed,
    branch,
    hidden,
    acc,
    part_out,
    part_in,
    squares,
    band,
    tile,
    sc_in,
    sc_sum,
    scale,
    inverses,
    g_send,
    g_recv,
    load_sem,
    p_recv,
    s_recv,
):
    me = spot()
    greet(me, False)
    t, other = me["t"], 1 - me["t"]
    here = (me["z"] % 2, me["y"], me["x"])
    bufs = (w0, w1, w2, w3, w4)
    gather = Gather(bufs, g_send, g_recv, me)

    def rows_of(i, size=BLOCK):
        return pl.ds(i * size, size)

    def scale_tile():
        place = me["z"] % 2 * 16 + me["y"] * 4 + me["x"]
        lane = lax.broadcasted_iota(jnp.int32, (1, 128), 1)
        base = 0
        for ref in (mix_s, group_s, up_s, down_s):
            n = ref.shape[1] // 2
            q = lax.broadcasted_iota(jnp.int32, (n, 2 * n), 0)
            r = lax.broadcasted_iota(jnp.int32, (n, 2 * n), 1)
            value = jnp.zeros((n, 128), F32)
            for j in range(2):
                for h in range(2):
                    own = jnp.where(r == 2 * q + h, ref[j : j + 1], 0.0)
                    column = jnp.sum(own, axis=1, keepdims=True)
                    value = value + jnp.where(lane == h * 64 + 2 * place + j, column, 0.0)
            tile[base : base + n] = value
            base += n

    def load(k, src, dst):
        copy = pltpu.make_async_copy(src, dst, load_sem.at[k])
        copy.start()
        return copy

    pairs = (
        (mix_in, mix_w),
        (group_in, group_w),
        (up_in, up_w),
        (down_in, down_w),
        (gains_in, gains),
        (mix_s_in, mix_s),
        (group_s_in, group_s),
        (up_s_in, up_s),
        (down_s_in, down_s),
    )
    early = [load(k, src, dst) for k, (src, dst) in enumerate(pairs)]
    own_tokens = load(len(pairs), tokens, x_buf.at[t])
    early[0].wait()
    w0[here[0], here[1], here[2], 0:64] = mix_w[...].astype(BF16)
    with jax.named_scope("greet"):
        greet(me, True)

    def share(kind, i, src, dst):
        gather.start((kind, i), src, dst, p_recv.at[kind, i], "t", other)

    def arrived(kind, i, ref):
        gather.arrived((kind, i), ref, p_recv.at[kind, i])

    for p in range(2):
        gather.tick(0, p, 0)
    share(0, 0, tokens, x_buf.at[t])

    for copy in early[5:]:
        copy.wait()
    scale_tile()
    early[1].wait()
    w0[here[0], here[1], here[2], 64:80, 0:GW] = group_w[0].astype(BF16)
    w0[here[0], here[1], here[2], 64:80, GW:] = group_w[1].astype(BF16)
    early[2].wait()
    up_all = up_w[...].astype(BF16)
    for ref, lane in ((w1, 0), (w2, 1024)):
        ref[here[0], here[1], here[2]] = up_all[:, lane : lane + 1024]
    early[3].wait()
    down_all = down_w[...].astype(BF16)
    for ref, lane in ((w3, 0), (w4, 1024)):
        ref[here[0], here[1], here[2]] = down_all[:, lane : lane + 1024]
    early[4].wait()

    def scales(step):
        if step == 0:
            for d in (1, 2, 3):
                at = lax.rem(me["x"] + d, 4)
                gather.start("sx", tile, sc_in.at[d - 1], s_recv.at[0], "x", at)
        if step == 1:
            gather.arrived("sx", sc_in.at[0:3], s_recv.at[0])
            sc_sum[0] = tile[...] + sc_in[0] + sc_in[1] + sc_in[2]
        if step == 2:
            for d in (1, 2, 3):
                at = lax.rem(me["y"] + d, 4)
                gather.start("sy", sc_sum.at[0], sc_in.at[d + 2], s_recv.at[1], "y", at)
        if step == 3:
            gather.arrived("sy", sc_in.at[3:6], s_recv.at[1])
            sc_sum[1] = sc_sum[0] + sc_in[3] + sc_in[4] + sc_in[5]
        if step == 4:
            at = me["z"] + 1 - 2 * (me["z"] % 2)
            gather.start("sz", sc_sum.at[1], sc_in.at[6], s_recv.at[2], "z", at)
        if step == 5:
            gather.arrived("sz", sc_in.at[6], s_recv.at[2])
            whole = sc_sum[1] + sc_in[6]
            for q in range(40):
                scale[q // 8 : q // 8 + 1, 128 * (q % 8) : 128 * (q % 8) + 128] = whole[q : q + 1]

    def bands():
        i = lax.broadcasted_iota(jnp.int32, (BLOCK, 2 * BLOCK), 0)
        j = lax.broadcasted_iota(jnp.int32, (BLOCK, 2 * BLOCK), 1) - BLOCK
        for g, window in enumerate((2 + 6 * t, 4 + 12 * t)):
            band[g] = jnp.where((j <= i) & (j > i - window), 1.0, 0.0).astype(BF16)

    def mean_inverse(total):
        return lax.rsqrt(total * (1.0 / (2 * HALF)) + EPS)

    def row_sum(v):
        return jnp.sum(v, axis=1, keepdims=True)

    SUB, UNROLL = 16, 4

    def first_norm(i):
        if i == 0:
            own_tokens.wait()
            arrived(0, 0, x_buf.at[other])
        g0, g1 = gains[0:1, 0:HALF], gains[0:1, HALF:]

        def body(k, _):
            rows = pl.ds(pl.multiple_of(i * BLOCK + k * SUB, SUB), SUB)
            a, b = x_buf[0, rows].astype(F32), x_buf[1, rows].astype(F32)
            inverse = mean_inverse(row_sum(a * a + b * b))
            normed[rows, 0:HALF] = (a * inverse * g0).astype(BF16)
            normed[rows, HALF:] = (b * inverse * g1).astype(BF16)
            return 0

        lax.fori_loop(0, BLOCK // SUB, body, 0, unroll=UNROLL)

    def mix(p):
        cols = slice(GW * p, GW * p + GW)
        weight = w0[:, :, :, 0:64, cols].reshape(2 * HALF, GW)
        mixed[:, cols] = (dot(normed[...], weight) * scale[0:1, cols]).astype(BF16)

    def pool(i):
        rows = slice(i * BLOCK, i * BLOCK + BLOCK)
        for g in range(2):
            cols = slice(GW * g, GW * g + GW)
            window = (2 + 6 * t, 4 + 12 * t)[g]
            own = mixed[rows, cols]
            if i == 0:
                sums = dot(band[g, :, BLOCK:], own)
                position = lax.broadcasted_iota(jnp.int32, (BLOCK, 1), 0)
                sums = sums / jnp.minimum(position + 1, window).astype(F32)
            else:
                sums = dot(band[g], mixed[rows.start - BLOCK : rows.stop, cols])
                sums = sums * (1.0 / jnp.full((BLOCK, 1), window, jnp.int32).astype(F32))
            pooled = (sums - own.astype(F32)).astype(BF16)
            weight = w0[:, :, :, 64:80, cols].reshape(GW, GW)
            branch[t, rows, cols] = (dot(pooled, weight) * scale[1:2, cols]).astype(BF16)

    def branch_share(i):
        share(1, i, branch.at[t, rows_of(i)], branch.at[t, rows_of(i)])

    def middle(i):
        arrived(1, i, branch.at[other, rows_of(i)])
        post = [gains[1:2, 0:HALF], gains[1:2, HALF:]]
        pre = [gains[2:3, 0:HALF], gains[2:3, HALF:]]

        def body(k, _):
            rows = pl.ds(pl.multiple_of(i * BLOCK + k * SUB, SUB), SUB)
            parts = [branch[h, rows].astype(F32) for h in range(2)]
            inverse = mean_inverse(row_sum(parts[0] * parts[0] + parts[1] * parts[1]))
            mids = []
            for h in range(2):
                add = (parts[h] * inverse * post[h]).astype(BF16).astype(F32)
                mid = (x_buf[h, rows].astype(F32) + add).astype(BF16)
                x_buf[h, rows] = mid
                mids.append(mid.astype(F32))
            inverse = mean_inverse(row_sum(mids[0] * mids[0] + mids[1] * mids[1]))
            for h in range(2):
                normed[rows, h * HALF : h * HALF + HALF] = (mids[h] * inverse * pre[h]).astype(BF16)
            return 0

        lax.fori_loop(0, BLOCK // SUB, body, 0, unroll=UNROLL)

    def up(buf, p):
        cols = slice(512 * p, 512 * p + 512)
        place = slice((buf - 1) * 1024 + 512 * p, (buf - 1) * 1024 + 512 * p + 512)
        weight = bufs[buf][:, :, :, :, cols].reshape(2 * HALF, 512)
        act = jnp.maximum(dot(normed[...], weight) * scale[buf + 1 : buf + 2, cols], 0.0)
        hidden[:, place] = (act * act).astype(BF16)

    def down(b, n, part=None):
        buf, lane, width = ((3, 0, 1024), (4, 0, KCUT), (4, KCUT, 1024 - KCUT))[b - 4]
        half, k = (other, n) if n < 2 else (t, n - 2)
        first = (buf - 3) * 1024 + lane
        weight = bufs[buf][half, 2 * k : 2 * k + 2, :, :, lane : lane + width]
        weight = weight.reshape(512, width)
        cols = slice(512 * k, 512 * k + 512)

        rows = ALL if part is None else pl.ds(part * MROWS, MROWS)
        value = dot_t(hidden[rows, first : first + width], weight)
        if buf > 3:
            value = value + acc[half, rows, cols]
        if b < NB - 1:
            acc[half, rows, cols] = value
        elif n < 2:
            part_out[rows, cols] = value.astype(BF16)
        else:
            mixed[rows, cols] = value.astype(BF16)

    def last(part):
        for n in range(2):
            down(NB - 1, n, part)
            place = (rows_of(part, 512), pl.ds(512 * n, 512))
            share(2, 2 * part + n, part_out.at[place], part_in.at[place])

    def last_own(part):
        for n in range(2, 4):
            down(NB - 1, n, part)

    def total(i):
        if i % 2 == 0:
            for n in range(2):
                arrived(2, i + n, part_in.at[rows_of(i // 2, 512), pl.ds(512 * n, 512)])

        def body(k, _):
            rows = pl.ds(pl.multiple_of(i * BLOCK + k * SUB, SUB), SUB)
            both = mixed[rows].astype(F32) + part_in[rows].astype(F32)
            value = (both * scale[4:5]).astype(BF16)
            mixed[rows] = value
            value = value.astype(F32)
            square = value * value
            lanes = square[:, 0:128]
            for q in range(1, 8):
                lanes = lanes + square[:, 128 * q : 128 * q + 128]
            squares[t, rows] = lanes
            return 0

        lax.fori_loop(0, BLOCK // SUB, body, 0, unroll=UNROLL)
        share(3, i, squares.at[t, rows_of(i)], squares.at[t, rows_of(i)])

    def final(i):
        arrived(3, i, squares.at[other, rows_of(i)])
        gain = gains[3:4, pl.ds(pl.multiple_of(t * HALF, HALF), HALF)]
        squared = squares[0, rows_of(i)] + squares[1, rows_of(i)]
        inverses[...] = jnp.broadcast_to(mean_inverse(row_sum(squared)), (BLOCK, 128))

        def body(k, _):
            at = pl.ds(pl.multiple_of(k * SUB, SUB), SUB)
            rows = pl.ds(pl.multiple_of(i * BLOCK + k * SUB, SUB), SUB)
            inverse = jnp.concatenate([inverses[at]] * (HALF // 128), axis=1)
            add = (mixed[rows].astype(F32) * inverse * gain).astype(BF16).astype(F32)
            out[rows] = (x_buf[t, rows].astype(F32) + add).astype(BF16)
            return 0

        lax.fori_loop(0, BLOCK // SUB, body, 0, unroll=UNROLL)

    def run(name, step, *args):
        with jax.named_scope(name):
            step(*args)

    steps = dict(
        sc=scales, bands=bands, norm=first_norm, mix=mix, pool=pool, mid=middle, up=up, dn=down
    )
    steps.update(T=gather.tick, share=branch_share, total=total, final=final)
    steps.update(last=last, own=last_own)
    run("sc", scales, 0)
    for name, *args in PLAN:
        run("#".join(map(str, (name, *args))), steps[name], *args)


def on_device(
    tokens,
    norm_gains,
    mix_weight,
    mix_scale,
    group_weight,
    group_scale,
    up_weight,
    up_scale,
    down_weight,
    down_scale,
):
    arrays = (tokens, norm_gains, mix_weight, group_weight, up_weight, down_weight.T)
    arrays += (mix_scale.T, group_scale.T, up_scale.T, down_scale.T)
    dma = pltpu.SemaphoreType.DMA
    return pl.pallas_call(
        kernel,
        out_shape=pltpu.VMEM((LENGTH, HALF), BF16),
        in_specs=[pl.BlockSpec(memory_space=pl.ANY)] + [pl.BlockSpec(memory_space=pl.ANY)] * 9,
        out_specs=pl.BlockSpec(memory_space=pltpu.VMEM),
        scratch_shapes=[pltpu.VMEM(a.shape, F32) for a in arrays[1:]]
        + [pltpu.VMEM((2, 4, 4, r, 1024), BF16) for r in ROWS]
        + [
            pltpu.VMEM((2, LENGTH, HALF), BF16),
            pltpu.VMEM((LENGTH, 2 * HALF), BF16),
            pltpu.VMEM((LENGTH, HALF), BF16),
            pltpu.VMEM((2, LENGTH, HALF), BF16),
            pltpu.VMEM((LENGTH, 2048), BF16),
            pltpu.VMEM((2, LENGTH, HALF), F32),
            pltpu.VMEM((LENGTH, HALF), BF16),
            pltpu.VMEM((LENGTH, HALF), BF16),
            pltpu.VMEM((2, LENGTH, 128), F32),
            pltpu.VMEM((2, BLOCK, 2 * BLOCK), BF16),
            pltpu.VMEM((40, 128), F32),
            pltpu.VMEM((7, 40, 128), F32),
            pltpu.VMEM((2, 40, 128), F32),
            pltpu.VMEM((5, 1024), F32),
            pltpu.VMEM((BLOCK, 128), F32),
            dma((POOL,)),
            dma((NB, 2, 5)),
            dma((10,)),
            dma((4, NR)),
            dma((3,)),
        ],
        compiler_params=pltpu.CompilerParams(
            collective_id=0, has_side_effects=True, vmem_limit_bytes=60_000_000
        ),
    )(*arrays)


def solution(mesh):
    finer = Mesh(
        mesh.devices.reshape(mesh.shape["rep"], 2, 4, 4, mesh.shape["tp"]),
        ("rep", "fs_0", "fs_1", "fs_2", "tp"),
    )
    in_specs = (
        P(REP_FS, "tp"),
        P(),
        P(FS, "tp"),
        P("tp", FS),
        P("tp", FS, None),
        P("tp", FS),
        P(FS, "tp"),
        P("tp", FS),
        P("tp", FS),
        P("tp", FS),
    )
    out_specs = P(REP_FS, "tp")
    return jax.shard_map(
        on_device, mesh=finer, in_specs=in_specs, out_specs=out_specs, check_vma=False
    )
```
